32 devices in a mesh: ep: 16 (over z, y, x), tp: 2 (over core).
Axes of the slice: x: 2, y: 2, z: 4, core: 2. Of those that a mesh axis runs over, the one named last changes fastest.
Arguments:
- tokens: bfloat16 [256, 2048], P('ep'), may hold values from -6 to 6
- norm_gain: float32 [2048], replicated, may hold values from 0.1 to 1.9
- query_weight: bfloat16 [2048, 1024], P('ep', 'tp'), may hold values from -0.125 to 0.125
- key_weight: bfloat16 [2048, 1024], P('ep', 'tp'), may hold values from -0.125 to 0.125
- value_weight: bfloat16 [2048, 1024], P('ep', 'tp'), may hold values from -0.125 to 0.125
- outgate_weight: bfloat16 [2048, 1024], P('ep', 'tp'), may hold values from -0.125 to 0.125
- input_weight: bfloat16 [2048, 8], P('ep', 'tp'), may hold values from -0.125 to 0.125
- forget_weight: bfloat16 [2048, 8], P('ep', 'tp'), may hold values from -0.125 to 0.125
- forget_bias: float32 [8], P('tp'), may hold values from -1 to 5
- memory: float32 [256, 8, 128, 128], P('ep', 'tp'), may hold values from -2.4 to 2.4
- stabilizer: float32 [256, 8], P('ep', 'tp'), may hold values from -3 to 3
- head_gain: float32 [1024], P('tp'), may hold values from 0.1 to 1.9
- mix_weight: bfloat16 [1024, 2048], P('tp', 'ep'), may hold values from -0.1875 to 0.1875
- second_gain: float32 [2048], replicated, may hold values from 0.1 to 1.9
- route_experts: int32 [256, 4], P('ep'), may hold values from 0 to 15, all different within a row; in each aligned block of 16 rows (0 to 15, 16 to 31, ...) at most 8 rows name the same one
- route_weight: float32 [256, 4], P('ep'), may hold values from 0.1 to 1
- expert_gate: bfloat16 [16, 2048, 2048], P('ep', None, 'tp'), may hold values from -0.5 to 0.5
- expert_up: bfloat16 [16, 2048, 2048], P('ep', None, 'tp'), may hold values from -0.5 to 0.5
- expert_down: bfloat16 [16, 2048, 2048], P('ep', 'tp'), may hold values from -0.03125 to 0.03125
- dense_gate: bfloat16 [4096, 2048], P(('ep', 'tp')), may hold values from -0.125 to 0.125
- dense_up: bfloat16 [4096, 2048], P(('ep', 'tp')), may hold values from -0.125 to 0.125
- dense_down: bfloat16 [4096, 2048], P(('ep', 'tp')), may hold values from -0.09375 to 0.09375
- branch_scale: float32 [2048], replicated, may hold values from 0.3 to 1.5
Outputs:
- mixed: bfloat16 [256, 2048], P('ep', 'tp')
- memory_new: float32 [256, 8, 128, 128], P('ep', 'tp')
- stabilizer_new: float32 [256, 8], P('ep', 'tp')
The draws below stay inside these ranges and needn't reach their ends.
Inputs may be any that keep to these rules, and one draw needn't show every extreme that they name: `route_experts`: each row names 4 different experts. Within each aligned block of 16 rows no expert is named by more than 8 rows, and in every draw some expert is named by exactly 8 rows of some block.
All inputs are finite; a program needn't handle non-finite values.
Results may differ from the reference program's by a relative error of at most 0.03.
Values may be sent and summed in bfloat16 or wider, within the bound.
A program may use at most 128 MiB of HBM per device.

```python
import math
import jax
import jax.numpy as jnp
import numpy as np
from jax import lax

MODEL = 2048
HEADS = 8
HEAD_SIZE = 128
HIDDEN_SIZE = 2048
DENSE = 4096
TOPK = 4
SEQ_GROUP = 16
BATCH = 256
EXPERTS = 16
CAPACITY = 8
N_EP = 16
N_TP = 2


def shard_levels(key, dims, shards, least, largest):
    def one(position, parts):
        steps = jax.random.uniform(jax.random.fold_in(jax.random.fold_in(key, 6), position), (parts,), jnp.float32, least / len(shards), largest / len(shards))
        return jnp.repeat(jnp.exp(steps), dims[position] // parts).reshape((-1,) + (1,) * (len(dims) - position - 1))

    level = one(*shards[0])
    for cut in shards[1:]:
        level = level * one(*cut)
    return level


def routed_block(rng, own, number, rows, count, top, most, lean):
    ranking = jax.random.permutation(rng, count)
    crowded, common = portions_of(count, rows * top, most, lean, True), portions_of(count, rows * top, most, lean, False)
    places = jnp.arange(count)

    def named(sizes, offset_by):
        used = int((sizes > 0).sum())
        fixed = max(1, used // 4)
        passed = fixed + (places - fixed + offset_by * (used - fixed)) % max(1, count - fixed)
        return jnp.zeros((count,), jnp.int32).at[ranking[jnp.where(places < fixed, places, passed)]].set(jnp.asarray(sizes, jnp.int32))

    sizes = jnp.where(number % 4 == 0, named(crowded, number // 4), named(common, number - number // 4 - 1))
    mixed = jax.random.permutation(jax.random.fold_in(own, 3), count)
    giver, receiver = mixed[0:count // 2 * 2:2], mixed[1:count // 2 * 2:2]
    margin = jnp.minimum(sizes[giver] - 1, most - sizes[receiver]) // 2
    margin = jnp.where((giver == ranking[0]) | (receiver == ranking[0]) | (sizes[receiver] == 0), 0, jnp.maximum(margin, 0))
    passed = jax.random.randint(jax.random.fold_in(own, 4), (count // 2,), 0, 1 << 20) % (margin + 1)
    sizes = sizes.at[giver].add(-passed).at[receiver].add(passed)
    members = jnp.searchsorted(jnp.cumsum(sizes), jnp.arange(rows * top), side="right").astype(jnp.int32)
    grid = members.reshape(top, rows).T
    grid = grid[jax.random.permutation(jax.random.fold_in(own, 1), rows)]
    offset_by = jax.random.randint(jax.random.fold_in(own, 2), (rows, 1), 0, top)
    return jnp.take_along_axis(grid, (jnp.arange(top)[None, :] + offset_by) % top, axis=1)


def portions_of(number_of, total, limit, slope, full):
    weights = [(1 << 20) // math.isqrt(rank ** slope) + 1 for rank in range(1, number_of + 1)]
    largest = limit if full else min(limit, max(-(-total // number_of), total * weights[0] // sum(weights)))
    least = 1 if total - largest >= number_of - 1 else 0
    given, rest = [largest] + [least] * (number_of - 1), total - largest - least * (number_of - 1)
    while rest > 0:
        candidates = [i for i in range(1, number_of) if given[i] < largest] or [i for i in range(1, number_of) if given[i] < limit]
        whole, budget = sum([weights[i] for i in candidates]), rest
        for i in candidates:
            addition = min(limit - given[i], max(1, budget * weights[i] // whole), rest)
            given[i] = given[i] + addition
            rest = rest - addition
    return np.array(given)


def gaussian(key, dims, scale, limit, shards=(), dtype=jnp.bfloat16):
    result = scale * jax.random.normal(key, dims, jnp.float32)
    if shards:
        result = result * shard_levels(key, dims, shards, -0.22, 0.18)
    return jnp.clip(result, -limit, limit).astype(dtype)


def setup_inputs(seed: int = 0) -> dict:
    arg_keys = jax.random.split(jax.random.key(seed), 24)
    tokens = gaussian(arg_keys[0], (BATCH, MODEL), 1.0, 6.0, ((0, 16),))
    norm_gain = jnp.clip(1.0 + 0.18 * jax.random.normal(arg_keys[1], (MODEL,), jnp.float32), 0.1, 1.9)
    query_weight = gaussian(arg_keys[2], (MODEL, HEADS * HEAD_SIZE), MODEL ** -0.5, 0.125, ((0, 16), (1, 2)))
    key_weight = gaussian(arg_keys[3], (MODEL, HEADS * HEAD_SIZE), MODEL ** -0.5, 0.125, ((0, 16), (1, 2)))
    value_weight = gaussian(arg_keys[4], (MODEL, HEADS * HEAD_SIZE), MODEL ** -0.5, 0.125, ((0, 16), (1, 2)))
    outgate_weight = gaussian(arg_keys[5], (MODEL, HEADS * HEAD_SIZE), MODEL ** -0.5, 0.125, ((0, 16), (1, 2)))
    input_weight = gaussian(arg_keys[6], (MODEL, HEADS), MODEL ** -0.5, 0.125, ((0, 16), (1, 2)))
    forget_weight = gaussian(arg_keys[7], (MODEL, HEADS), MODEL ** -0.5, 0.125, ((0, 16), (1, 2)))
    forget_bias = jnp.clip(-1.0 + 6.0 * jax.random.uniform(arg_keys[8], (HEADS,), jnp.float32) ** shard_levels(arg_keys[8], (HEADS,), ((0, 2),), -0.2, 0.2), -1.0, 5.0)
    memory = gaussian(arg_keys[9], (BATCH, HEADS, HEAD_SIZE, HEAD_SIZE), 0.3, 2.4, ((0, 16), (1, 2)), jnp.float32)
    stabilizer = jnp.clip(jax.random.uniform(arg_keys[10], (BATCH, HEADS), jnp.float32, -3.0, 3.0) * shard_levels(arg_keys[10], (BATCH, HEADS), ((0, 16), (1, 2)), -0.4, 0.0), -3.0, 3.0)
    head_gain = jnp.clip(1.0 + 0.18 * jax.random.normal(arg_keys[11], (HEADS * HEAD_SIZE,), jnp.float32), 0.1, 1.9)
    mix_weight = gaussian(arg_keys[12], (HEADS * HEAD_SIZE, MODEL), (HEADS * HEAD_SIZE) ** -0.5, 0.1875, ((0, 2), (1, 16)))
    second_gain = jnp.clip(1.0 + 0.18 * jax.random.normal(arg_keys[13], (MODEL,), jnp.float32), 0.1, 1.9)
    route_experts_keys = jax.random.split(jax.random.fold_in(arg_keys[14], 1), BATCH // SEQ_GROUP)
    route_experts_turns = jax.random.permutation(jax.random.fold_in(arg_keys[14], 3), BATCH // SEQ_GROUP)
    route_experts = jax.vmap(lambda own, number: routed_block(jax.random.fold_in(arg_keys[14], 2), own, number, SEQ_GROUP, EXPERTS, TOPK, CAPACITY, 2))(route_experts_keys, route_experts_turns).reshape((BATCH, TOPK))
    route_weight = jnp.clip(jnp.exp(math.log(1.0) - 2.3025851 * jax.random.uniform(arg_keys[15], (BATCH, TOPK), jnp.float32) ** shard_levels(arg_keys[15], (BATCH, TOPK), ((0, 16),), -0.2, 0.2)), 0.1, 1.0)
    expert_gate = gaussian(arg_keys[16], (EXPERTS, MODEL, HIDDEN_SIZE), (MODEL // 16) ** -0.5, 0.5, ((0, 16), (2, 2)))
    expert_up = gaussian(arg_keys[17], (EXPERTS, MODEL, HIDDEN_SIZE), (MODEL // 16) ** -0.5, 0.5, ((0, 16), (2, 2)))
    expert_down = gaussian(arg_keys[18], (EXPERTS, HIDDEN_SIZE, MODEL), (16 * HIDDEN_SIZE) ** -0.5, 0.03125, ((0, 16), (1, 2)))
    dense_gate = gaussian(arg_keys[19], (DENSE, MODEL), MODEL ** -0.5, 0.125, ((0, 32),))
    dense_up = gaussian(arg_keys[20], (DENSE, MODEL), MODEL ** -0.5, 0.125, ((0, 32),))
    dense_down = gaussian(arg_keys[21], (DENSE, MODEL), DENSE ** -0.5, 0.09375, ((0, 32),))
    branch_scale = jnp.clip(jax.random.uniform(arg_keys[22], (MODEL,), jnp.float32, 0.3, 1.5), 0.3, 1.5)
    return dict(tokens=tokens, norm_gain=norm_gain, query_weight=query_weight, key_weight=key_weight, value_weight=value_weight, outgate_weight=outgate_weight, input_weight=input_weight, forget_weight=forget_weight, forget_bias=forget_bias, memory=memory, stabilizer=stabilizer, head_gain=head_gain, mix_weight=mix_weight, second_gain=second_gain, route_experts=route_experts, route_weight=route_weight, expert_gate=expert_gate, expert_up=expert_up, expert_down=expert_down, dense_gate=dense_gate, dense_up=dense_up, dense_down=dense_down, branch_scale=branch_scale)


norm_eps = 1e-05
clamp_limit = 7.0
sigmoid_slope = 1.702

def rms_scale(values, gain):
    mean_square = lax.optimization_barrier(jnp.mean(values * values, axis=-1, keepdims=True))
    return values * lax.rsqrt(mean_square + norm_eps) * gain

def round_half(values):
    return lax.optimization_barrier(values.astype(jnp.bfloat16)).astype(jnp.float32)

def clamped_unit(gate_pre, up_pre):
    gate_clamped = jnp.minimum(gate_pre, clamp_limit)
    up_clamped = jnp.clip(up_pre, -clamp_limit, clamp_limit)
    return ((up_clamped + 1.0) * gate_clamped * jax.nn.sigmoid(sigmoid_slope * gate_clamped)).astype(jnp.bfloat16)

def memory_step(projected, forget_bias, memory, stabilizer, head_gain):
    query_rows, key_rows, value_rows, outgate_rows, input_pre, forget_pre = projected
    sequences, head_count = stabilizer.shape
    head_size = memory.shape[-1]
    log_forget = jax.nn.log_sigmoid(forget_pre + forget_bias)
    stab_new = jnp.maximum(log_forget + stabilizer, input_pre)
    carried = jnp.exp(log_forget + stabilizer - stab_new)
    written = jnp.exp(input_pre - stab_new)
    query_heads = query_rows.astype(jnp.float32).reshape(sequences, head_count, head_size)
    key_heads = key_rows.astype(jnp.float32).reshape(sequences, head_count, head_size) * head_size ** (-0.5)
    value_heads = value_rows.astype(jnp.float32).reshape(sequences, head_count, head_size)
    memory_new = carried[:, :, None, None] * memory + written[:, :, None, None] * value_heads[:, :, :, None] * key_heads[:, :, None, :]
    readout = jnp.einsum('bhvk,bhk->bhv', memory_new, query_heads, precision=lax.Precision.HIGHEST)
    out_gate = jax.nn.sigmoid(outgate_rows.astype(jnp.float32).reshape(sequences, head_count, head_size))
    gated = (rms_scale(readout, head_gain.reshape(head_count, head_size)) * out_gate).astype(jnp.bfloat16)
    return (gated.reshape(sequences, head_count * head_size), memory_new, stab_new)

def expert_mix(normed_second, route_experts, route_weight, expert_gate, expert_up, expert_down):
    batch_rows, model_width = normed_second.shape
    expert_count = expert_gate.shape[0]
    hidden_units = expert_gate.shape[2]
    group_units = hidden_units // N_TP
    blocks = normed_second.astype(jnp.float32).reshape(N_EP, batch_rows // N_EP, model_width)
    slots = jnp.arange(CAPACITY).astype(jnp.float32)

    def one_expert(total, index):
        matched = route_experts == index
        hit_mask = jnp.any(matched, axis=1).astype(jnp.float32).reshape(N_EP, -1)
        weights = lax.optimization_barrier(jnp.sum(jnp.where(matched, route_weight, 0.0), axis=1)).reshape(N_EP, -1)
        ranks = jnp.cumsum(hit_mask, axis=1) - 1.0
        select = hit_mask[:, None, :] * (ranks[:, None, :] == slots[None, :, None]).astype(jnp.float32)
        rows = jnp.einsum('jcs,jsd->jcd', select, blocks, precision=lax.Precision.HIGHEST)
        rows = rows.astype(jnp.bfloat16).reshape(-1, model_width)
        gate_pre = jnp.dot(rows, expert_gate[index], preferred_element_type=jnp.float32)
        up_pre = jnp.dot(rows, expert_up[index], preferred_element_type=jnp.float32)
        activity = clamped_unit(gate_pre, up_pre)
        down_weight = expert_down[index]
        outputs = jnp.zeros((rows.shape[0], model_width), jnp.float32)
        for group in range(N_TP):
            lower = group * group_units
            outputs = outputs + round_half(jnp.dot(activity[:, lower:lower + group_units], down_weight[lower:lower + group_units], preferred_element_type=jnp.float32))
        outputs = outputs.reshape(N_EP, CAPACITY, model_width)
        spread = jnp.einsum('jcs,jcd->jsd', select * weights[:, None, :], outputs, precision=lax.Precision.HIGHEST)
        return (total + spread.reshape(batch_rows, model_width), None)
    total, unused = lax.scan(one_expert, jnp.zeros((batch_rows, model_width), jnp.float32), jnp.arange(expert_count).astype(jnp.int32))
    return total

def reference(tokens, norm_gain, query_weight, key_weight, value_weight, outgate_weight, input_weight, forget_weight, forget_bias, memory, stabilizer, head_gain, mix_weight, second_gain, route_experts, route_weight, expert_gate, expert_up, expert_down, dense_gate, dense_up, dense_down, branch_scale):
    inputs_float = tokens.astype(jnp.float32)
    normed = rms_scale(inputs_float, norm_gain).astype(jnp.bfloat16)
    projected = (jnp.dot(normed, query_weight, preferred_element_type=jnp.float32).astype(jnp.bfloat16), jnp.dot(normed, key_weight, preferred_element_type=jnp.float32).astype(jnp.bfloat16), jnp.dot(normed, value_weight, preferred_element_type=jnp.float32).astype(jnp.bfloat16), jnp.dot(normed, outgate_weight, preferred_element_type=jnp.float32).astype(jnp.bfloat16), jnp.dot(normed, input_weight, preferred_element_type=jnp.float32), jnp.dot(normed, forget_weight, preferred_element_type=jnp.float32))
    gated, memory_new, stab_new = memory_step(projected, forget_bias, memory, stabilizer, head_gain)
    group_width = gated.shape[1] // N_TP
    attended = jnp.zeros_like(inputs_float)
    for group in range(N_TP):
        lower = group * group_width
        attended = attended + round_half(jnp.dot(gated[:, lower:lower + group_width], mix_weight[lower:lower + group_width], preferred_element_type=jnp.float32))
    residual = (inputs_float + attended).astype(jnp.bfloat16)
    residual_float = residual.astype(jnp.float32)
    normed_second = rms_scale(residual_float, second_gain).astype(jnp.bfloat16)
    routed = expert_mix(normed_second, route_experts, route_weight, expert_gate, expert_up, expert_down)
    dense_pre = jnp.dot(normed_second, dense_gate.T, preferred_element_type=jnp.float32)
    dense_lift = jnp.dot(normed_second, dense_up.T, preferred_element_type=jnp.float32)
    dense_act = (jax.nn.silu(dense_pre) * dense_lift).astype(jnp.bfloat16)
    dense_out = jnp.dot(dense_act, dense_down, preferred_element_type=jnp.float32)
    mixed = (residual_float + routed + branch_scale * dense_out).astype(jnp.bfloat16)
    return (mixed, memory_new, stab_new)
```

```python
import functools

import jax
import jax.numpy as jnp
from jax import lax
from jax.experimental import pallas as pl
from jax.experimental.pallas import tpu as pltpu
from jax.sharding import PartitionSpec as P

norm_eps = 1e-05
clamp_limit = 7.0
sigmoid_slope = 1.702
lanes = 128
f32 = jnp.float32
bf16 = jnp.bfloat16


def loop(lower, upper, step):
    def run(index, carry):
        step(index)
        return carry

    lax.fori_loop(lower, upper, run, 0)


def remote(source, landing, send_sem, recv_sem, **target):
    return pltpu.make_async_remote_copy(
        src_ref=source,
        dst_ref=landing,
        send_sem=send_sem,
        recv_sem=recv_sem,
        device_id=target,
        device_id_type=pl.DeviceIdType.MESH,
    )


def greet(barrier, **target):
    pl.semaphore_signal(
        barrier, inc=1, device_id=target, device_id_type=pl.DeviceIdType.MESH
    )


class Place:
    def __init__(self, outer, inner):
        self.outer, self.inner = outer, inner
        self.me = lax.axis_index("ep")
        self.side = lax.axis_index("tp")
        self.o = self.me // inner
        self.n = self.me % inner

    def plane(self, step):
        return (self.o + step) % self.outer

    def spot(self, step):
        return (self.n + step) % self.inner

    def at(self, plane, spot):
        return plane * self.inner + spot


def gather(place, slot, send_sem, recv_sem, arrived):
    outer, inner, me = place.outer, place.inner, place.me

    def copy(source, target):
        return remote(
            slot(source), slot(source), send_sem, recv_sem.at[source], ep=target
        )

    loop(1, outer, lambda t: copy(me, place.at(place.plane(t), place.n)).start())
    loop(1, inner, lambda u: copy(me, place.at(place.o, place.spot(u))).start())
    arrived(me)

    def relay(t):
        source = place.at(place.plane(t), place.n)
        copy(source, source).wait_recv()
        loop(
            1,
            inner,
            lambda u: copy(source, place.at(place.o, place.spot(u))).start(),
        )
        arrived(source)

    loop(1, outer, relay)

    def take(t):
        def one(u):
            source = place.at(place.plane(t), place.spot(u))
            copy(source, source).wait_recv()
            arrived(source)

        loop(1, inner, one)

    loop(0, outer, take)


def sigmoid(values):
    return 1.0 / (1.0 + jnp.exp(-values))


def first_kernel(
    outer,
    inner,
    tok_in,
    norm_gain_in,
    wq,
    wk,
    wv,
    wo,
    wi_in,
    wf_in,
    bias_in,
    stab_in,
    head_gain_in,
    mix_in,
    rexp_in,
    rwt_in,
    mem_in,
    res,
    rww,
    stab_out,
    mem,
    tok,
    norm_gain,
    wide,
    wi,
    wf,
    bias,
    stab,
    hgain,
    mix,
    rexp,
    rwt,
    nbuf,
    nland,
    tbuf,
    tland,
    rbuf,
    pg,
    gland1,
    gmid,
    gland2,
    pbuf,
    land1,
    mid,
    land2,
    mid_half,
    land2_half,
    turned,
    carried_rows,
    written_rows,
    gland,
    pv,
    came,
    in_s,
    wide_s,
    p1_s,
    p1_r,
    tk_s,
    tk_r,
    rt_s,
    rt_r,
    g1_s,
    g1_r,
    g2_s,
    g2_r,
    l1_s,
    l1_r,
    l2_s,
    l2_r,
    l3_s,
    l3_r,
    mi,
    ag_s,
    ag_r,
    ap_r,
    tp_s,
    tp_r,
    ar_s,
    ar_r,
    sb_s,
    sb_r,
):
    place = Place(outer, inner)
    me, side, o, n = place.me, place.side, place.o, place.n
    count = outer * inner
    sequences, heads, size = mem.shape[0], mem.shape[1], mem.shape[2]
    width = nland.shape[2]
    rows = count * sequences
    half = pv.shape[1]
    per_half = count // 2
    sibling = 1 - side

    barrier = pltpu.get_barrier_semaphore()
    loop(1, count, lambda t: greet(barrier, ep=(me + t) % count))
    greet(barrier, tp=sibling)
    small = [
        pltpu.make_async_copy(source, target, in_s.at[i])
        for i, (source, target) in enumerate(
            (
                (tok_in, tok),
                (norm_gain_in, norm_gain),
                (rexp_in, rexp),
                (rwt_in, rwt),
                (wi_in, wi),
                (wf_in, wf),
                (bias_in, bias),
                (stab_in, stab),
                (head_gain_in, hgain),
                (mix_in, mix),
            )
        )
    ]
    for copy in small[:6]:
        copy.start()

    def wide_copies(h):
        part = slice(h * size, (h + 1) * size)
        return [
            pltpu.make_async_copy(
                weight.at[:, part],
                wide.at[h, :, slice(j * size, (j + 1) * size)],
                wide_s.at[4 * h + j],
            )
            for j, weight in enumerate((wq, wk, wv, wo))
        ]

    for h in range(heads):
        for copy in wide_copies(h):
            copy.start()
    for copy in small[6:]:
        copy.start()
    loop(
        0,
        heads,
        lambda h: pltpu.make_async_copy(mem_in.at[:, h], mem.at[:, h], mi.at[h]).start(),
    )

    small[0].wait()
    small[1].wait()
    tokens = tok[...].astype(f32)
    mean_square = jnp.mean(tokens * tokens, axis=-1, keepdims=True)
    normed = (tokens * lax.rsqrt(mean_square + norm_eps) * norm_gain[...]).astype(bf16)
    for p in range(count):
        nbuf[p] = normed[:, p * width : (p + 1) * width]
        tbuf[p] = tok[:, p * width : (p + 1) * width]

    small[2].wait()
    small[3].wait()
    topk = rexp.shape[0]
    experts = lax.broadcasted_iota(jnp.int32, (count, sequences), 0)
    weights = jnp.zeros((count, sequences), f32)
    for k in range(topk):
        weights += jnp.where(rexp[k : k + 1, :] == experts, rwt[k : k + 1, :], 0.0)
    rbuf[...] = jnp.zeros_like(rbuf)
    for p in range(count):
        rbuf[p, :, :sequences] = weights[p : p + 1, :]

    with jax.named_scope("barrier"):
        pl.semaphore_wait(barrier, count)

    def send_normed(t):
        peer = (me + t) % count
        remote(nbuf.at[peer], nland.at[me], p1_s, p1_r, ep=peer).start()

    loop(1, count, send_normed)
    mine = side == me // per_half

    def token_copy(t):
        peer = (me + t) % count
        return remote(
            tbuf.at[peer], tland.at[me % per_half], tk_s, tk_r.at[me % per_half], ep=peer
        )

    @pl.when(mine)
    def _():
        loop(1, count, lambda t: token_copy(t).start())
        tland[me % per_half] = tbuf[me]

    def send_route(t):
        peer = (me + t) % count
        remote(rbuf.at[peer], rww.at[me], rt_s, rt_r, ep=peer).start()

    loop(1, count, send_route)
    rww[me] = rbuf[me]
    nland[me] = nbuf[me]

    small[4].wait()
    small[5].wait()
    gates = 2 * heads
    once = jnp.concatenate((wi[...].astype(f32), wf[...].astype(f32)), axis=0)
    thin = jnp.concatenate(
        (once, once, jnp.zeros((lanes - 2 * gates, width), f32)), axis=0
    ).astype(bf16)

    with jax.named_scope("normed"):
        others = nland.at[pl.ds(0, count - 1)]
        remote(others, others, p1_s, p1_r, ep=me).wait_recv()
    columns = nland[...].reshape(rows, width)

    lane = lax.broadcasted_iota(jnp.int32, (rows, lanes), 1)
    thin_sums = lax.dot_general(
        columns, thin, (((1,), (1,)), ((), ())), preferred_element_type=f32
    )
    upper = thin_sums.astype(bf16).astype(f32)
    parted = jnp.where(lane < gates, upper, thin_sums - upper).astype(bf16)
    pg[...] = parted.reshape(outer, inner, sequences, lanes)

    def send_gates(t):
        spot = place.spot(t)
        remote(
            pg.at[:, spot], gland1.at[n], g1_s, g1_r, ep=place.at(o, spot)
        ).start()

    loop(1, inner, send_gates)

    def send_part(h, plane):
        def send(t):
            spot = place.spot(t)
            remote(
                pbuf.at[h, plane, spot],
                land1.at[h, plane, n],
                l1_s,
                l1_r.at[h * outer + plane],
                ep=place.at(o, spot),
            ).start()

        loop(1, inner, send)

    for h in range(heads):
        for copy in wide_copies(h):
            copy.wait()
        sums = jnp.dot(columns, wide[h], preferred_element_type=f32).astype(bf16)
        pbuf[h] = sums.reshape(outer, inner, sequences, 4 * size)
        loop(1, outer, lambda t: send_part(h, place.plane(t)))
        if h > 0:
            send_part(h - 1, o)
    send_part(heads - 1, o)
    for copy in small[6:]:
        copy.wait()

    with jax.named_scope("gates"):
        others = gland1.at[pl.ds(0, inner - 1)]
        remote(others, others, g1_s, g1_r, ep=me).wait_recv()
    for a in range(outer):
        total = pg[a, n].astype(f32)
        for t in range(1, inner):
            total += gland1[place.spot(t), a].astype(f32)
        gmid[a] = total

    def pass_gates(t):
        plane = place.plane(t)
        remote(
            gmid.at[plane], gland2.at[o], g2_s, g2_r, ep=place.at(plane, n)
        ).start()

    loop(1, outer, pass_gates)

    def plane_sum(h, plane):
        with jax.named_scope("first"):
            others = land1.at[h, plane, pl.ds(0, inner - 1)]
            remote(others, others, l1_s, l1_r.at[h * outer + plane], ep=me).wait_recv()
        total = pbuf[h, plane, n].astype(f32)
        for t in range(1, inner):
            total += land1[h, plane, place.spot(t)].astype(f32)
        return total

    def first_sum(h):
        def send(t):
            plane = place.plane(t)
            total = plane_sum(h, plane)
            mid[h, plane] = total[:, : 2 * size]
            mid_half[h, plane] = total[:, 2 * size :].astype(bf16)
            target = place.at(plane, n)
            remote(mid.at[h, plane], land2.at[h, o], l2_s, l2_r.at[h], ep=target).start()
            remote(
                mid_half.at[h, plane], land2_half.at[h, o], l3_s, l3_r.at[h], ep=target
            ).start()

        loop(1, outer, send)

    def gate_math():
        with jax.named_scope("gates2"):
            others = gland2.at[pl.ds(0, outer - 1)]
            remote(others, others, g2_s, g2_r, ep=me).wait_recv()
        total = gmid[o]
        for t in range(1, outer):
            total += gland2[place.plane(t)]
        turn = jnp.transpose(total)
        turn = turn[:gates] + turn[gates : 2 * gates]
        input_pre, forget_pre = turn[:heads], turn[heads:]
        square = lax.broadcasted_iota(jnp.int32, (heads, heads), 0) == lax.broadcasted_iota(
            jnp.int32, (heads, heads), 1
        )
        shift = jnp.sum(jnp.where(square, bias[...], 0.0), axis=1, keepdims=True)
        shifted = forget_pre + shift
        log_forget = jnp.minimum(shifted, 0.0) - jnp.log1p(jnp.exp(-jnp.abs(shifted)))
        stab_new = jnp.maximum(log_forget + stab[...], input_pre)
        stab_out[...] = stab_new
        turned[...] = jnp.zeros_like(turned)
        turned[:heads, :sequences] = jnp.exp(log_forget + stab[...] - stab_new)
        turned[heads:gates, :sequences] = jnp.exp(input_pre - stab_new)
        back = jnp.transpose(turned[...])[:sequences]
        for h in range(heads):
            carried_rows[h] = jnp.broadcast_to(back[:, h : h + 1], (sequences, lanes))
            written_rows[h] = jnp.broadcast_to(
                back[:, heads + h : heads + h + 1], (sequences, lanes)
            )

    def memory_head(h):
        own = plane_sum(h, o)
        with jax.named_scope("heads"):
            others = land2.at[h, pl.ds(0, outer - 1)]
            remote(others, others, l2_s, l2_r.at[h], ep=me).wait_recv()
            others = land2_half.at[h, pl.ds(0, outer - 1)]
            remote(others, others, l3_s, l3_r.at[h], ep=me).wait_recv()
        pltpu.make_async_copy(mem_in.at[:, h], mem.at[:, h], mi.at[h]).wait()
        query_key, value_gate = own[:, : 2 * size], own[:, 2 * size :]
        for t in range(1, outer):
            query_key += land2[h, place.plane(t)]
            value_gate += land2_half[h, place.plane(t)].astype(f32)
        query_key = query_key.astype(bf16).astype(f32)
        value_gate = value_gate.astype(bf16).astype(f32)
        query = query_key[:, :size]
        key = query_key[:, size:] * size**-0.5 * written_rows[h]
        value = value_gate[:, :size]
        outgate = value_gate[:, size:]
        carry = carried_rows[h]
        value_columns = jnp.transpose(value)
        places = lax.broadcasted_iota(jnp.int32, (size, lanes), 1)
        readout_columns = jnp.zeros((size, lanes), f32)
        for s in range(sequences):
            updated = (
                carry[s : s + 1, :] * mem[s, h] + value_columns[:, s : s + 1] * key[s : s + 1, :]
            )
            mem[s, h] = updated
            column = jnp.sum(updated * query[s : s + 1, :], axis=1, keepdims=True)
            readout_columns = jnp.where(places == s, column, readout_columns)
        readout = jnp.transpose(readout_columns)[:sequences]
        mean_square = jnp.mean(readout * readout, axis=-1, keepdims=True)
        gated = (
            readout
            * lax.rsqrt(mean_square + norm_eps)
            * hgain[h : h + 1, :]
            * sigmoid(outgate)
        )
        gland[h, me] = gated.astype(bf16)
        block = gland.at[h, me]
        loop(
            1,
            outer,
            lambda t: remote(
                block, block, ag_s, ag_r.at[h], ep=place.at(place.plane(t), n)
            ).start(),
        )
        loop(
            1,
            inner,
            lambda u: remote(
                block, block, ag_s, ap_r.at[h], ep=place.at(o, place.spot(u))
            ).start(),
        )

    def relay(h):
        others = gland.at[h, pl.ds(0, outer - 1)]
        remote(others, others, ag_s, ag_r.at[h], ep=me).wait_recv()

        def one(t):
            block = gland.at[h, place.at(place.plane(t), n)]
            loop(
                1,
                inner,
                lambda u: remote(
                    block, block, ag_s, ap_r.at[h], ep=place.at(o, place.spot(u))
                ).start(),
            )

        loop(1, outer, one)

    first_sum(0)
    gate_math()

    def both(h):
        first_sum(h)
        memory_head(h - 1)

        if h > 1:
            relay(h - 2)

    for h in range(1, heads):
        both(h)
    memory_head(heads - 1)

    with jax.named_scope("gated"):
        if heads > 1:
            relay(heads - 2)
        relay(heads - 1)
        partial = jnp.zeros((rows, width), f32)
        for h in range(heads):
            others = gland.at[h, pl.ds(0, outer * (inner - 1))]
            remote(others, others, ag_s, ap_r.at[h], ep=me).wait_recv()
            partial += jnp.dot(
                gland[h].reshape(rows, size),
                mix[h * size : (h + 1) * size, :],
                preferred_element_type=f32,
            )
        partial = partial.astype(bf16)
    pv[...] = partial.reshape(2, half, width)
    swap = remote(pv.at[sibling], came, tp_s, tp_r, tp=sibling)
    swap.start()

    def take_tokens(b):
        source = side * per_half + b

        @pl.when(source != me)
        def _():
            remote(tland.at[b], tland.at[b], tk_s, tk_r.at[b], ep=source).wait_recv()

    loop(0, per_half, take_tokens)
    with jax.named_scope("swap"):
        swap.wait_recv()
    attended = pv[side].astype(f32) + came[...].astype(f32)
    residual = (tland[...].reshape(half, width).astype(f32) + attended).astype(bf16)
    if len(res.shape) == 3:
        res[side, :, pl.ds(pl.multiple_of(me * width, width), width)] = residual
    else:
        res[me, side] = residual

    def slot(p, core):
        if len(res.shape) == 3:
            return res.at[core, :, pl.ds(pl.multiple_of(p * width, width), width)]
        return res.at[p, core]

    def hand(p):
        remote(slot(p, side), slot(p, side), sb_s, sb_r, tp=sibling).start()

    with jax.named_scope("rows"):
        gather(place, lambda p: slot(p, side), ar_s, ar_r, hand)

    with jax.named_scope("settle"):
        if len(res.shape) == 3:
            whole, sent = res.at[sibling], res.at[side, :, pl.ds(0, (count - 1) * width)]
        else:
            whole, sent = res.at[:, sibling], res.at[pl.ds(0, count - 1), side]
        remote(whole, whole, sb_s, sb_r, tp=sibling).wait()

    remote(sent, sent, ar_s, ar_r.at[0], ep=me).wait_send()
    others = rww.at[pl.ds(0, count - 1)]
    remote(others, others, rt_s, rt_r, ep=me).wait()
    others = nbuf.at[pl.ds(0, count - 1)]
    remote(others, others, p1_s, p1_r, ep=me).wait_send()

    @pl.when(mine)
    def _():
        remote(others, others, tk_s, tk_r.at[0], ep=me).wait_send()

    others = gland1.at[pl.ds(0, inner - 1)]
    remote(others, others, g1_s, g1_r, ep=me).wait_send()
    others = gmid.at[pl.ds(0, outer - 1)]
    remote(others, others, g2_s, g2_r, ep=me).wait_send()
    others = pbuf.at[:, :, pl.ds(0, inner - 1)]
    remote(others, others, l1_s, l1_r.at[0], ep=me).wait_send()
    others = mid.at[:, pl.ds(0, outer - 1)]
    remote(others, others, l2_s, l2_r.at[0], ep=me).wait_send()
    others = mid_half.at[:, pl.ds(0, outer - 1)]
    remote(others, others, l3_s, l3_r.at[0], ep=me).wait_send()
    others = gland.at[:, pl.ds(0, count - 1)]
    remote(others, others, ag_s, ag_r.at[0], ep=me).wait_send()
    swap.wait_send()


def second_kernel(
    outer,
    inner,
    chunks,
    row_blocks,
    res,
    rww,
    gain_in,
    scale_in,
    wg,
    wu,
    wd,
    dg,
    du,
    dd,
    out,
    gain,
    scale,
    wgv,
    wuv,
    wdv,
    dgv,
    duv,
    ddv,
    normed,
    dense_act,
    row_weight,
    act,
    passed,
    landed,
    kept,
    summed,
    land1,
    mid,
    land2,
    wg_m,
    wu_m,
    wd_m,
    d_m,
    tp_s,
    tp_r,
    l1_s,
    l1_r,
    l2_s,
    l2_r,
):
    place = Place(outer, inner)
    me, side, o, n = place.me, place.side, place.o, place.n
    count = outer * inner
    rows, model_width = normed.shape
    sequences = rows // count
    sibling = 1 - side
    hidden_chunk = wgv.shape[2]
    column_chunk = wdv.shape[2]
    part_width = chunks * column_chunk

    barrier = pltpu.get_barrier_semaphore()
    loop(1, inner, lambda u: greet(barrier, ep=place.at(o, place.spot(u))))
    loop(1, outer, lambda t: greet(barrier, ep=place.at(place.plane(t), n)))
    greet(barrier, tp=sibling)

    dense = [
        pltpu.make_async_copy(source, target, d_m.at[i])
        for i, (source, target) in enumerate(
            ((dg, dgv), (du, duv), (dd, ddv), (gain_in, gain), (scale_in, scale))
        )
    ]
    hidden_chunks = wgv.shape[0]

    def gate_copy(c):
        span = pl.ds(c * hidden_chunk, hidden_chunk)
        return pltpu.make_async_copy(wg.at[0, :, span], wgv.at[c], wg_m.at[c])

    def up_copy(c):
        span = pl.ds(c * hidden_chunk, hidden_chunk)
        return pltpu.make_async_copy(wu.at[0, :, span], wuv.at[c], wu_m.at[c])

    def down_copy(c):
        span = pl.ds(c * column_chunk, column_chunk)
        return pltpu.make_async_copy(wd.at[0, :, span], wdv.at[c], wd_m.at[c])

    dense[3].start()
    dense[0].start()
    dense[1].start()
    for c in range(hidden_chunks):
        gate_copy(c).start()
        up_copy(c).start()
    dense[2].start()
    dense[4].start()
    for c in range(chunks):
        down_copy(sibling * chunks + c).start()
        down_copy(side * chunks + c).start()

    block = act.shape[0] // row_blocks

    def norm_rows(r):
        span = pl.ds(pl.multiple_of(r * norm_block, norm_block), norm_block)
        values = res[span, :].astype(f32)
        mean_square = jnp.mean(values * values, axis=-1, keepdims=True)
        normed[span, :] = (values * lax.rsqrt(mean_square + norm_eps) * gain[...]).astype(bf16)

    norm_block = min(rows, 32)
    dense[3].wait()
    with jax.named_scope("norm"):
        loop(0, rows // norm_block, norm_rows)
    received = jnp.broadcast_to(rww[...], (count, sequences, lanes)).reshape(rows, lanes)
    line = lax.broadcasted_iota(jnp.int32, (rows, lanes), 0) % sequences
    lane = lax.broadcasted_iota(jnp.int32, (rows, lanes), 1)
    row_weight[...] = jnp.sum(jnp.where(line == lane, received, 0.0), axis=-1, keepdims=True)

    against = (((1,), (1,)), ((), ()))
    dense[0].wait()
    dense[1].wait()

    def part(r):
        return pl.ds(pl.multiple_of(r * block, block), block)

    def dense_rows(r):
        gate_rows = lax.dot_general(
            normed[part(r), :], dgv[...], against, preferred_element_type=f32
        )
        lift_rows = lax.dot_general(
            normed[part(r), :], duv[...], against, preferred_element_type=f32
        )
        dense_act[part(r), :] = (gate_rows * sigmoid(gate_rows) * lift_rows).astype(bf16)

    with jax.named_scope("dense"):
        loop(0, row_blocks, dense_rows)

    def hidden_step(c):
        gate_copy(c).wait()
        up_copy(c).wait()

        def one(r):
            gate_pre = jnp.dot(normed[part(r), :], wgv[c], preferred_element_type=f32)
            up_pre = jnp.dot(normed[part(r), :], wuv[c], preferred_element_type=f32)
            gate_pre = jnp.minimum(gate_pre, clamp_limit)
            up_pre = jnp.clip(up_pre, -clamp_limit, clamp_limit)
            span = pl.ds(pl.multiple_of(c * hidden_chunk, hidden_chunk), hidden_chunk)
            act[part(r), span] = (
                (up_pre + 1.0) * gate_pre * sigmoid(sigmoid_slope * gate_pre)
            ).astype(bf16)

        loop(0, row_blocks, one)

    with jax.named_scope("hidden"):
        loop(0, hidden_chunks, hidden_step)

    dense[2].wait()
    dense[4].wait()
    pl.semaphore_wait(barrier, inner + outer - 1)

    def term(c, r):
        span = pl.ds(pl.multiple_of(c * column_chunk, column_chunk), column_chunk)
        routed = jnp.dot(act[part(r), :], wdv[c], preferred_element_type=f32)
        dense_out = jnp.dot(dense_act[part(r), :], ddv[:, span], preferred_element_type=f32)
        return dense_out * scale[:, span] + row_weight[part(r), :] * routed

    def cross(c):
        return remote(passed.at[c], landed.at[c], tp_s, tp_r.at[c], tp=sibling)

    def spread_plane(c, plane):
        def send(t):
            spot = place.spot(t)
            remote(
                summed.at[c, plane, spot],
                land1.at[c, plane, n],
                l1_s,
                l1_r.at[c * outer + plane],
                ep=place.at(o, spot),
            ).start()

        loop(1, inner, send)

    def spread(c):
        cross(c).wait_recv()
        both = kept[c] + landed[c].astype(f32)
        summed[c] = both.astype(bf16).reshape(outer, inner, sequences, column_chunk)

        loop(1, outer, lambda t: spread_plane(c, place.plane(t)))

    def give_step(c):
        down_copy(sibling * chunks + c).wait()

        def give(r):
            passed[c, part(r), :] = term(sibling * chunks + c, r).astype(bf16)

        loop(0, row_blocks, give)
        cross(c).start()

    def keep_step(c):
        down_copy(side * chunks + c).wait()

        def keep(r):
            kept[c, part(r), :] = term(side * chunks + c, r)

        loop(0, row_blocks, keep)
        spread(c)

    with jax.named_scope("give"):
        loop(0, chunks, give_step)
    with jax.named_scope("keep"):
        loop(0, chunks, keep_step)

    loop(0, chunks, lambda c: spread_plane(c, o))

    def plane_sum(c, plane):
        others = land1.at[c, plane, pl.ds(0, inner - 1)]
        remote(others, others, l1_s, l1_r.at[c * outer + plane], ep=me).wait_recv()
        total = summed[c, plane, n].astype(f32)
        for t in range(1, inner):
            total += land1[c, plane, place.spot(t)].astype(f32)
        return total

    def first_sum(c):
        def send(t):
            plane = place.plane(t)
            mid[c, plane] = plane_sum(c, plane).astype(bf16)
            remote(
                mid.at[c, plane], land2.at[c, o], l2_s, l2_r.at[c], ep=place.at(plane, n)
            ).start()

        loop(1, outer, send)

    with jax.named_scope("sum1"):
        loop(0, chunks, first_sum)

    residual = res[
        pl.ds(pl.multiple_of(me * sequences, sequences), sequences),
        pl.ds(pl.multiple_of(side * part_width, part_width), part_width),
    ].astype(f32)

    with jax.named_scope("sum2"):
        for c in range(chunks):
            total = plane_sum(c, o)
            others = land2.at[c, pl.ds(0, outer - 1)]
            remote(others, others, l2_s, l2_r.at[c], ep=me).wait_recv()
            for t in range(1, outer):
                total += land2[c, place.plane(t)].astype(f32)
            span = slice(c * column_chunk, (c + 1) * column_chunk)
            out[:, span] = (residual[:, span] + total).astype(bf16)

    remote(passed, landed, tp_s, tp_r.at[0], tp=sibling).wait_send()
    others = summed.at[:, :, pl.ds(0, inner - 1)]
    remote(others, others, l1_s, l1_r.at[0], ep=me).wait_send()
    others = mid.at[:, pl.ds(0, outer - 1)]
    remote(others, others, l2_s, l2_r.at[0], ep=me).wait_send()


def last_kernel(mixed_in, memory_in, stab_in, mixed, memory, stab, sems):
    pairs = ((memory_in, memory), (mixed_in, mixed), (stab_in, stab))
    moves = [
        pltpu.make_async_copy(source, target, sems.at[i])
        for i, (source, target) in enumerate(pairs)
    ]
    for move in moves:
        move.start()
    for move in moves:
        move.wait()


def in_vmem():
    return pl.BlockSpec(memory_space=pltpu.VMEM)


def in_place():
    return pl.BlockSpec(memory_space=pltpu.HBM)


def held(*arrays):
    return [pltpu.with_memory_space_constraint(array, pltpu.HBM) for array in arrays]


def copies(*numbers):
    return [
        pltpu.SemaphoreType.DMA((number,)) if number else pltpu.SemaphoreType.DMA
        for number in numbers
    ]


def body(
    tokens,
    norm_gain,
    query_weight,
    key_weight,
    value_weight,
    outgate_weight,
    input_weight,
    forget_weight,
    forget_bias,
    memory,
    stabilizer,
    head_gain,
    mix_weight,
    second_gain,
    route_experts,
    route_weight,
    expert_gate,
    expert_up,
    expert_down,
    dense_gate,
    dense_up,
    dense_down,
    branch_scale,
):
    sequences, model_width = tokens.shape
    count = lax.axis_size("ep")
    sides = lax.axis_size("tp")
    inner = 1 << ((count.bit_length() - 1) // 2)
    outer = count // inner
    rows = sequences * count
    half = rows // sides
    width = model_width // count
    heads, size = memory.shape[1], memory.shape[2]
    head_width = query_weight.shape[1]
    part_width = model_width // sides
    topk = route_experts.shape[1]

    aligned = width % lanes == 0
    landing = (sides, half, model_width) if aligned else (count, sides, half, width)
    gates = 2 * heads
    grown = rows // 256

    residual, row_weights, stab_new, memory_new = pl.pallas_call(
        functools.partial(first_kernel, outer, inner),
        out_shape=(
            jax.ShapeDtypeStruct(landing, bf16),
            jax.ShapeDtypeStruct((count, 1, lanes), f32),
            jax.ShapeDtypeStruct((heads, sequences), f32),
            jax.ShapeDtypeStruct(memory.shape, f32),
        ),
        in_specs=[in_place()] * 15,
        out_specs=(in_vmem(),) * 4,
        scratch_shapes=[
            pltpu.VMEM((sequences, model_width), bf16),
            pltpu.VMEM((1, model_width), f32),
            pltpu.VMEM((heads, width, 4 * size), bf16),
            pltpu.VMEM((heads, width), bf16),
            pltpu.VMEM((heads, width), bf16),
            pltpu.VMEM((1, heads), f32),
            pltpu.VMEM((heads, sequences), f32),
            pltpu.VMEM((heads, size), f32),
            pltpu.VMEM((head_width, width), bf16),
            pltpu.VMEM((topk, sequences), jnp.int32),
            pltpu.VMEM((topk, sequences), f32),
            pltpu.VMEM((count, sequences, width), bf16),
            pltpu.VMEM((count, sequences, width), bf16),
            pltpu.VMEM((count, sequences, width), bf16),
            pltpu.VMEM((count // sides, sequences, width), bf16),
            pltpu.VMEM((count, 1, lanes), f32),
            pltpu.VMEM((outer, inner, sequences, lanes), bf16),
            pltpu.VMEM((inner, outer, sequences, lanes), bf16),
            pltpu.VMEM((outer, sequences, lanes), f32),
            pltpu.VMEM((outer, sequences, lanes), f32),
            pltpu.VMEM((heads, outer, inner, sequences, 4 * size), bf16),
            pltpu.VMEM((heads, outer, inner, sequences, 4 * size), bf16),
            pltpu.VMEM((heads, outer, sequences, 2 * size), f32),
            pltpu.VMEM((heads, outer, sequences, 2 * size), f32),
            pltpu.VMEM((heads, outer, sequences, 2 * size), bf16),
            pltpu.VMEM((heads, outer, sequences, 2 * size), bf16),
            pltpu.VMEM((gates, lanes), f32),
            pltpu.VMEM((heads, sequences, lanes), f32),
            pltpu.VMEM((heads, sequences, lanes), f32),
            pltpu.VMEM((heads, count, sequences, size), bf16),
            pltpu.VMEM((sides, half, width), bf16),
            pltpu.VMEM((half, width), bf16),
        ]
        + copies(10, 4 * heads)
        + copies(0, 0, 0, count // sides, 0, 0, 0, 0, 0, 0)
        + copies(0, heads * outer, 0, heads, 0, heads, heads)
        + copies(0, heads, heads, 0, 0, 0, count, 0, 0),
        compiler_params=pltpu.CompilerParams(
            collective_id=1, has_side_effects=True, vmem_limit_bytes=(14 + 8 * grown) * 2**20
        ),
    )(
        *held(
        tokens,
        norm_gain.reshape(1, model_width),
        query_weight,
        key_weight,
        value_weight,
        outgate_weight,
        input_weight.T,
        forget_weight.T,
        forget_bias.reshape(1, heads),
        stabilizer.T,
        head_gain.reshape(heads, size),
        mix_weight,
        route_experts.T,
        route_weight.T,
        memory,
        )
    )
    if not aligned:
        residual = residual.transpose(1, 2, 0, 3)
    residual = residual.reshape(rows, model_width)

    hidden = expert_gate.shape[2]
    dense_rows = dense_gate.shape[0]
    hidden_chunk = min(hidden, 256)
    column_chunk = min(part_width, 256)
    chunks = part_width // column_chunk
    mixed = pl.pallas_call(
        functools.partial(second_kernel, outer, inner, chunks, max(1, rows // 256)),
        out_shape=jax.ShapeDtypeStruct((sequences, part_width), bf16),
        in_specs=[in_vmem()] * 2 + [in_place()] * 8,
        out_specs=in_vmem(),
        scratch_shapes=[
            pltpu.VMEM((1, model_width), f32),
            pltpu.VMEM((1, model_width), f32),
            pltpu.VMEM((hidden // hidden_chunk, model_width, hidden_chunk), bf16),
            pltpu.VMEM((hidden // hidden_chunk, model_width, hidden_chunk), bf16),
            pltpu.VMEM((2 * chunks, hidden, column_chunk), bf16),
            pltpu.VMEM((dense_rows, model_width), bf16),
            pltpu.VMEM((dense_rows, model_width), bf16),
            pltpu.VMEM((dense_rows, model_width), bf16),
            pltpu.VMEM((rows, model_width), bf16),
            pltpu.VMEM((rows, dense_rows), bf16),
            pltpu.VMEM((rows, 1), f32),
            pltpu.VMEM((rows, hidden), bf16),
            pltpu.VMEM((chunks, rows, column_chunk), bf16),
            pltpu.VMEM((chunks, rows, column_chunk), bf16),
            pltpu.VMEM((chunks, rows, column_chunk), f32),
            pltpu.VMEM((chunks, outer, inner, sequences, column_chunk), bf16),
            pltpu.VMEM((chunks, outer, inner, sequences, column_chunk), bf16),
            pltpu.VMEM((chunks, outer, sequences, column_chunk), bf16),
            pltpu.VMEM((chunks, outer, sequences, column_chunk), bf16),
        ]
        + copies(hidden // hidden_chunk, hidden // hidden_chunk, 2 * chunks, 5)
        + copies(0, chunks, 0, chunks * outer, 0, chunks),
        compiler_params=pltpu.CompilerParams(
            collective_id=2, has_side_effects=True, vmem_limit_bytes=(20 + 8 * grown) * 2**20
        ),
    )(
        residual,
        row_weights,
        *held(
            second_gain.reshape(1, model_width),
            branch_scale.reshape(1, model_width),
            expert_gate,
            expert_up,
            expert_down,
            dense_gate,
            dense_up,
            dense_down,
        ),
    )
    mixed, memory_new, stab_new = pl.pallas_call(
        last_kernel,
        out_shape=tuple(
            jax.ShapeDtypeStruct(array.shape, array.dtype)
            for array in (mixed, memory_new, stab_new)
        ),
        in_specs=[in_vmem()] * 3,
        out_specs=(in_place(),) * 3,
        scratch_shapes=copies(3),
        compiler_params=pltpu.CompilerParams(vmem_limit_bytes=8 * 2**20),
    )(mixed, memory_new, stab_new)
    return (mixed, memory_new, stab_new.T)


def solution(mesh):
    in_specs = (
        P("ep", None),
        P(),
        P("ep", "tp"),
        P("ep", "tp"),
        P("ep", "tp"),
        P("ep", "tp"),
        P("ep", "tp"),
        P("ep", "tp"),
        P("tp"),
        P("ep", "tp", None, None),
        P("ep", "tp"),
        P("tp"),
        P("tp", "ep"),
        P(),
        P("ep", None),
        P("ep", None),
        P("ep", None, "tp"),
        P("ep", None, "tp"),
        P("ep", "tp", None),
        P(("ep", "tp"), None),
        P(("ep", "tp"), None),
        P(("ep", "tp"), None),
        P(),
    )
    out_specs = (P("ep", "tp"), P("ep", "tp", None, None), P("ep", "tp"))
    return jax.shard_map(body, mesh=mesh, in_specs=in_specs, out_specs=out_specs, check_vma=False)
```

```python
import functools

import jax
import jax.numpy as jnp
from jax import lax
from jax.experimental import pallas as pl
from jax.experimental.pallas import tpu as pltpu
from jax.sharding import PartitionSpec as P

norm_eps = 1e-05
clamp_limit = 7.0
sigmoid_slope = 1.702
lanes = 128
f32 = jnp.float32
bf16 = jnp.bfloat16


def loop(lower, upper, step):
    def run(index, carry):
        step(index)
        return carry

    lax.fori_loop(lower, upper, run, 0)


def remote(source, landing, send_sem, recv_sem, **target):
    return pltpu.make_async_remote_copy(
        src_ref=source,
        dst_ref=landing,
        send_sem=send_sem,
        recv_sem=recv_sem,
        device_id=target,
        device_id_type=pl.DeviceIdType.MESH,
    )


def greet(barrier, **target):
    pl.semaphore_signal(
        barrier, inc=1, device_id=target, device_id_type=pl.DeviceIdType.MESH
    )


class Place:
    def __init__(self, outer, inner):
        self.outer, self.inner = outer, inner
        self.me = lax.axis_index("ep")
        self.side = lax.axis_index("tp")
        self.o = self.me // inner
        self.n = self.me % inner

    def plane(self, step):
        return (self.o + step) % self.outer

    def spot(self, step):
        return (self.n + step) % self.inner

    def at(self, plane, spot):
        return plane * self.inner + spot


def gather(place, slot, send_sem, recv_sem, arrived, complete):
    outer, inner, me = place.outer, place.inner, place.me

    def copy(source, target):
        return remote(
            slot(source), slot(source), send_sem, recv_sem.at[source], ep=target
        )

    loop(1, outer, lambda t: copy(me, place.at(place.plane(t), place.n)).start())
    loop(1, inner, lambda u: copy(me, place.at(place.o, place.spot(u))).start())
    arrived(me)

    def relay(t):
        source = place.at(place.plane(t), place.n)
        copy(source, source).wait_recv()
        loop(
            1,
            inner,
            lambda u: copy(source, place.at(place.o, place.spot(u))).start(),
        )
        arrived(source)

    loop(1, outer, relay)

    def take(t):
        def one(u):
            source = place.at(place.plane(t), place.spot(u))
            copy(source, source).wait_recv()
            arrived(source)

        loop(1, inner, one)

    take(0)

    def turn(t):
        take(t)
        complete(t - 1)

    loop(1, outer, turn)
    complete(outer - 1)


def sigmoid(values):
    return 1.0 / (1.0 + jnp.exp(-values))


def first_kernel(
    outer,
    inner,
    tok_in,
    norm_gain_in,
    wq,
    wk,
    wv,
    wo,
    wi_in,
    wf_in,
    bias_in,
    stab_in,
    head_gain_in,
    mix_in,
    rexp_in,
    rwt_in,
    mem_in,
    res,
    rww,
    stab_out,
    mem,
    tok,
    norm_gain,
    wide,
    wi,
    wf,
    bias,
    stab,
    hgain,
    mix,
    rexp,
    rwt,
    nbuf,
    nland,
    tbuf,
    tland,
    rbuf,
    pg,
    gland1,
    gmid,
    gland2,
    pbuf,
    land1,
    mid,
    land2,
    mid_half,
    land2_half,
    turned,
    carried_rows,
    written_rows,
    gland,
    pv,
    came,
    in_s,
    wide_s,
    p1_s,
    p1_r,
    tk_s,
    tk_r,
    rt_s,
    rt_r,
    g1_s,
    g1_r,
    g2_s,
    g2_r,
    l1_s,
    l1_r,
    l2_s,
    l2_r,
    l3_s,
    l3_r,
    mi,
    ag_s,
    ag_r,
    ap_r,
    tp_s,
    tp_r,
    ar_s,
    ar_r,
    sb_s,
    sb_r,
    begin=lambda: None,
    ready=lambda: None,
    group=None,
):
    place = Place(outer, inner)
    me, side, o, n = place.me, place.side, place.o, place.n
    count = outer * inner
    sequences, heads, size = mem.shape[0], mem.shape[1], mem.shape[2]
    width = nland.shape[2]
    rows = count * sequences
    half = pv.shape[1]
    per_half = count // 2
    sibling = 1 - side

    barrier = pltpu.get_barrier_semaphore()
    loop(1, count, lambda t: greet(barrier, ep=(me + t) % count))
    greet(barrier, tp=sibling)
    small = [
        pltpu.make_async_copy(source, target, in_s.at[i])
        for i, (source, target) in enumerate(
            (
                (tok_in, tok),
                (norm_gain_in, norm_gain),
                (rexp_in, rexp),
                (rwt_in, rwt),
                (wi_in, wi),
                (wf_in, wf),
                (bias_in, bias),
                (stab_in, stab),
                (head_gain_in, hgain),
                (mix_in, mix),
            )
        )
    ]
    for copy in small[:6]:
        copy.start()

    def wide_copies(h):
        part = slice(h * size, (h + 1) * size)
        return [
            pltpu.make_async_copy(
                weight.at[:, part],
                wide.at[h, :, slice(j * size, (j + 1) * size)],
                wide_s.at[4 * h + j],
            )
            for j, weight in enumerate((wq, wk, wv, wo))
        ]

    for h in range(heads):
        for copy in wide_copies(h):
            copy.start()
    for copy in small[6:]:
        copy.start()
    loop(
        0,
        heads,
        lambda h: pltpu.make_async_copy(mem_in.at[:, h], mem.at[:, h], mi.at[h]).start(),
    )

    small[0].wait()
    small[1].wait()
    tokens = tok[...].astype(f32)
    mean_square = jnp.mean(tokens * tokens, axis=-1, keepdims=True)
    normed = (tokens * lax.rsqrt(mean_square + norm_eps) * norm_gain[...]).astype(bf16)
    for p in range(count):
        nbuf[p] = normed[:, p * width : (p + 1) * width]

    with jax.named_scope("barrier"):
        pl.semaphore_wait(barrier, count)

    def send_normed(t):
        peer = (me + t) % count
        remote(nbuf.at[peer], nland.at[me], p1_s, p1_r, ep=peer).start()

    loop(1, count, send_normed)
    nland[me] = nbuf[me]

    small[2].wait()
    small[3].wait()
    topk = rexp.shape[0]
    experts = lax.broadcasted_iota(jnp.int32, (count, sequences), 0)
    weights = jnp.zeros((count, sequences), f32)
    for k in range(topk):
        weights += jnp.where(rexp[k : k + 1, :] == experts, rwt[k : k + 1, :], 0.0)
    rbuf[...] = jnp.zeros_like(rbuf)
    for p in range(count):
        rbuf[p, :, :sequences] = weights[p : p + 1, :]

    for p in range(count):
        tbuf[p] = tok[:, p * width : (p + 1) * width]
    begin()
    mine = side == me // per_half

    def token_copy(t):
        peer = (me + t) % count
        return remote(
            tbuf.at[peer], tland.at[me % per_half], tk_s, tk_r.at[me % per_half], ep=peer
        )

    @pl.when(mine)
    def _():
        loop(1, count, lambda t: token_copy(t).start())
        tland[me % per_half] = tbuf[me]

    def send_route(t):
        peer = (me + t) % count
        remote(rbuf.at[peer], rww.at[me], rt_s, rt_r, ep=peer).start()

    loop(1, count, send_route)
    rww[me] = rbuf[me]

    small[4].wait()
    small[5].wait()
    gates = 2 * heads
    once = jnp.concatenate((wi[...].astype(f32), wf[...].astype(f32)), axis=0)
    thin = jnp.concatenate(
        (once, once, jnp.zeros((lanes - 2 * gates, width), f32)), axis=0
    ).astype(bf16)

    with jax.named_scope("normed"):
        others = nland.at[pl.ds(0, count - 1)]
        remote(others, others, p1_s, p1_r, ep=me).wait_recv()
    columns = nland[...].reshape(rows, width)

    lane = lax.broadcasted_iota(jnp.int32, (rows, lanes), 1)
    thin_sums = lax.dot_general(
        columns, thin, (((1,), (1,)), ((), ())), preferred_element_type=f32
    )
    upper = thin_sums.astype(bf16).astype(f32)
    parted = jnp.where(lane < gates, upper, thin_sums - upper).astype(bf16)
    pg[...] = parted.reshape(outer, inner, sequences, lanes)

    def send_gates(t):
        spot = place.spot(t)
        remote(
            pg.at[:, spot], gland1.at[n], g1_s, g1_r, ep=place.at(o, spot)
        ).start()

    loop(1, inner, send_gates)

    def send_part(h, plane):
        def send(t):
            spot = place.spot(t)
            remote(
                pbuf.at[h, plane, spot],
                land1.at[h, plane, n],
                l1_s,
                l1_r.at[h * outer + plane],
                ep=place.at(o, spot),
            ).start()

        loop(1, inner, send)

    for h in range(heads):
        for copy in wide_copies(h):
            copy.wait()
        sums = jnp.dot(columns, wide[h], preferred_element_type=f32).astype(bf16)
        pbuf[h] = sums.reshape(outer, inner, sequences, 4 * size)
        loop(1, outer, lambda t: send_part(h, place.plane(t)))
        if h > 0:
            send_part(h - 1, o)
    send_part(heads - 1, o)
    for copy in small[6:]:
        copy.wait()

    with jax.named_scope("gates"):
        others = gland1.at[pl.ds(0, inner - 1)]
        remote(others, others, g1_s, g1_r, ep=me).wait_recv()
    for a in range(outer):
        total = pg[a, n].astype(f32)
        for t in range(1, inner):
            total += gland1[place.spot(t), a].astype(f32)
        gmid[a] = total

    def pass_gates(t):
        plane = place.plane(t)
        remote(
            gmid.at[plane], gland2.at[o], g2_s, g2_r, ep=place.at(plane, n)
        ).start()

    loop(1, outer, pass_gates)

    def plane_sum(h, plane):
        with jax.named_scope("first"):
            others = land1.at[h, plane, pl.ds(0, inner - 1)]
            remote(others, others, l1_s, l1_r.at[h * outer + plane], ep=me).wait_recv()
        total = pbuf[h, plane, n].astype(f32)
        for t in range(1, inner):
            total += land1[h, plane, place.spot(t)].astype(f32)
        return total

    def first_sum(h):
        def send(t):
            plane = place.plane(t)
            total = plane_sum(h, plane)
            mid[h, plane] = total[:, : 2 * size]
            mid_half[h, plane] = total[:, 2 * size :].astype(bf16)
            target = place.at(plane, n)
            remote(mid.at[h, plane], land2.at[h, o], l2_s, l2_r.at[h], ep=target).start()
            remote(
                mid_half.at[h, plane], land2_half.at[h, o], l3_s, l3_r.at[h], ep=target
            ).start()

        loop(1, outer, send)

    def gate_math():
        with jax.named_scope("gates2"):
            others = gland2.at[pl.ds(0, outer - 1)]
            remote(others, others, g2_s, g2_r, ep=me).wait_recv()
        total = gmid[o]
        for t in range(1, outer):
            total += gland2[place.plane(t)]
        turn = jnp.transpose(total)
        turn = turn[:gates] + turn[gates : 2 * gates]
        input_pre, forget_pre = turn[:heads], turn[heads:]
        square = lax.broadcasted_iota(jnp.int32, (heads, heads), 0) == lax.broadcasted_iota(
            jnp.int32, (heads, heads), 1
        )
        shift = jnp.sum(jnp.where(square, bias[...], 0.0), axis=1, keepdims=True)
        shifted = forget_pre + shift
        log_forget = jnp.minimum(shifted, 0.0) - jnp.log1p(jnp.exp(-jnp.abs(shifted)))
        stab_new = jnp.maximum(log_forget + stab[...], input_pre)
        stab_out[...] = stab_new
        turned[...] = jnp.zeros_like(turned)
        turned[:heads, :sequences] = jnp.exp(log_forget + stab[...] - stab_new)
        turned[heads:gates, :sequences] = jnp.exp(input_pre - stab_new) * size**-0.5
        back = jnp.transpose(turned[...])[:sequences]
        for h in range(heads):
            carried_rows[h] = jnp.broadcast_to(back[:, h : h + 1], (sequences, lanes))
            written_rows[h] = jnp.broadcast_to(
                back[:, heads + h : heads + h + 1], (sequences, lanes)
            )

    def memory_head(h):
        own = plane_sum(h, o)
        with jax.named_scope("heads"):
            others = land2.at[h, pl.ds(0, outer - 1)]
            remote(others, others, l2_s, l2_r.at[h], ep=me).wait_recv()
            others = land2_half.at[h, pl.ds(0, outer - 1)]
            remote(others, others, l3_s, l3_r.at[h], ep=me).wait_recv()
        pltpu.make_async_copy(mem_in.at[:, h], mem.at[:, h], mi.at[h]).wait()
        query_key, value_gate = own[:, : 2 * size], own[:, 2 * size :]
        for t in range(1, outer):
            query_key += land2[h, place.plane(t)]
            value_gate += land2_half[h, place.plane(t)].astype(f32)
        query_key = query_key.astype(bf16)
        value_gate = value_gate.astype(bf16).astype(f32)
        query, key = query_key[:, :size], query_key[:, size:]
        value, outgate = value_gate[:, :size], value_gate[:, size:]
        value_columns = jnp.transpose(value)
        places = lax.broadcasted_iota(jnp.int32, (size, sequences), 1)
        lines = lax.broadcasted_iota(jnp.int32, (sequences, size), 0)
        across = (((1,), (1,)), ((), ()))

        def some(group, readout):
            for i in range(unroll):
                s = group * unroll + i
                column = jnp.where(places == s, value_columns, 0.0).astype(bf16)
                product = jnp.dot(column, key, preferred_element_type=f32)
                carry = carried_rows[h, pl.ds(s, 1), :]
                write = written_rows[h, pl.ds(s, 1), :]
                updated = carry * mem[s, h] + write * product
                mem[s, h] = updated
                upper = updated.astype(bf16)
                under = (updated - upper.astype(f32)).astype(bf16)
                answers = lax.dot_general(query, upper, across, preferred_element_type=f32)
                answers += lax.dot_general(query, under, across, preferred_element_type=f32)
                readout = jnp.where(lines == s, answers, readout)
            return readout

        unroll = min(sequences, 8)
        readout = lax.fori_loop(
            0, sequences // unroll, some, jnp.zeros((sequences, size), f32)
        )
        mean_square = jnp.mean(readout * readout, axis=-1, keepdims=True)
        gated = (
            readout
            * lax.rsqrt(mean_square + norm_eps)
            * hgain[pl.ds(h, 1), :]
            * sigmoid(outgate)
        )
        gland[h, me] = gated.astype(bf16)
        block = gland.at[h, me]
        loop(
            1,
            outer,
            lambda t: remote(
                block, block, ag_s, ag_r.at[h], ep=place.at(place.plane(t), n)
            ).start(),
        )
        loop(
            1,
            inner,
            lambda u: remote(
                block, block, ag_s, ap_r.at[h], ep=place.at(o, place.spot(u))
            ).start(),
        )

    def relay(h):
        others = gland.at[h, pl.ds(0, outer - 1)]
        remote(others, others, ag_s, ag_r.at[h], ep=me).wait_recv()

        def one(t):
            block = gland.at[h, place.at(place.plane(t), n)]
            loop(
                1,
                inner,
                lambda u: remote(
                    block, block, ag_s, ap_r.at[h], ep=place.at(o, place.spot(u))
                ).start(),
            )

        loop(1, outer, one)

    def head_step(h):
        @pl.when(h < heads)
        def _():
            first_sum(h)

        @pl.when(h == 0)
        def _():
            gate_math()

        @pl.when(h > 0)
        def _():
            memory_head(h - 1)

    loop(0, heads + 1, head_step)

    with jax.named_scope("gated"):
        loop(0, heads, relay)
        partial = jnp.zeros((rows, width), f32)
        for h in range(heads):
            others = gland.at[h, pl.ds(0, outer * (inner - 1))]
            remote(others, others, ag_s, ap_r.at[h], ep=me).wait_recv()
            partial += jnp.dot(
                gland[h].reshape(rows, size),
                mix[h * size : (h + 1) * size, :],
                preferred_element_type=f32,
            )
        partial = partial.astype(bf16)
    pv[...] = partial.reshape(2, half, width)
    swap = remote(pv.at[sibling], came, tp_s, tp_r, tp=sibling)
    swap.start()

    def take_tokens(b):
        source = side * per_half + b

        @pl.when(source != me)
        def _():
            remote(tland.at[b], tland.at[b], tk_s, tk_r.at[b], ep=source).wait_recv()

    loop(0, per_half, take_tokens)
    with jax.named_scope("swap"):
        swap.wait_recv()
    attended = pv[side].astype(f32) + came[...].astype(f32)
    residual = (tland[...].reshape(half, width).astype(f32) + attended).astype(bf16)
    def slot(p, core):
        if len(res.shape) == 2:
            return res.at[
                pl.ds(pl.multiple_of(core * half, half), half),
                pl.ds(pl.multiple_of(p * width, width), width),
            ]
        return res.at[p, core]

    slot(me, side)[...] = residual

    def hand(p):
        remote(slot(p, side), slot(p, side), sb_s, sb_r.at[p // inner], tp=sibling).start()

    def complete(t):
        plane = place.plane(t)
        if len(res.shape) == 2:
            across = pl.ds(pl.multiple_of(plane * inner * width, inner * width), inner * width)
            whole = res.at[pl.ds(pl.multiple_of(sibling * half, half), half), across]
        else:
            whole = res.at[pl.ds(plane * inner, inner), sibling]
        with jax.named_scope("settle"):
            remote(whole, whole, sb_s, sb_r.at[plane], tp=sibling).wait_recv()
        if group is not None:
            group(plane)

    ready()
    others = rww.at[pl.ds(0, count - 1)]
    remote(others, others, rt_s, rt_r, ep=me).wait()
    with jax.named_scope("rows"):
        gather(place, lambda p: slot(p, side), ar_s, ar_r, hand, complete)

    def settle():
        if len(res.shape) == 2:
            rows_side = pl.ds(pl.multiple_of(side * half, half), half)
            whole, sent = res.at[rows_side], res.at[rows_side, pl.ds(0, (count - 1) * width)]
        else:
            whole, sent = res.at[:, side], res.at[pl.ds(0, count - 1), side]
        remote(whole, whole, sb_s, sb_r.at[0], tp=sibling).wait_send()
        remote(sent, sent, ar_s, ar_r.at[0], ep=me).wait_send()
        others = nbuf.at[pl.ds(0, count - 1)]
        remote(others, others, p1_s, p1_r, ep=me).wait_send()

        @pl.when(mine)
        def _():
            remote(others, others, tk_s, tk_r.at[0], ep=me).wait_send()

        others = gland1.at[pl.ds(0, inner - 1)]
        remote(others, others, g1_s, g1_r, ep=me).wait_send()
        others = gmid.at[pl.ds(0, outer - 1)]
        remote(others, others, g2_s, g2_r, ep=me).wait_send()
        others = pbuf.at[:, :, pl.ds(0, inner - 1)]
        remote(others, others, l1_s, l1_r.at[0], ep=me).wait_send()
        others = mid.at[:, pl.ds(0, outer - 1)]
        remote(others, others, l2_s, l2_r.at[0], ep=me).wait_send()
        others = mid_half.at[:, pl.ds(0, outer - 1)]
        remote(others, others, l3_s, l3_r.at[0], ep=me).wait_send()
        others = gland.at[:, pl.ds(0, count - 1)]
        remote(others, others, ag_s, ag_r.at[0], ep=me).wait_send()
        swap.wait_send()

    return settle


def second_kernel(
    outer,
    inner,
    chunks,
    row_blocks,
    res,
    rww,
    gain_in,
    scale_in,
    wg,
    wu,
    wd,
    dg,
    du,
    dd,
    out,
    gain,
    scale,
    wgv,
    wuv,
    wdv,
    dgv,
    duv,
    ddv,
    gate_sum,
    up_sum,
    dense_gate_sum,
    dense_up_sum,
    squares,
    dense_act,
    row_weight,
    act,
    passed,
    landed,
    kept,
    summed,
    land1,
    mid,
    land2,
    wg_m,
    wu_m,
    wd_m,
    d_m,
    tp_s,
    tp_r,
    l1_s,
    l1_r,
    l2_s,
    l2_r,
):
    place = Place(outer, inner)
    me, side, o, n = place.me, place.side, place.o, place.n
    count = outer * inner
    rows, model_width = res.shape
    sequences = rows // count
    sibling = 1 - side
    hidden_chunk = wgv.shape[2]
    column_chunk = wdv.shape[2]
    part_width = chunks * column_chunk

    dense = [
        pltpu.make_async_copy(source, target, d_m.at[i])
        for i, (source, target) in enumerate(
            ((dg, dgv), (du, duv), (dd, ddv), (gain_in, gain), (scale_in, scale))
        )
    ]
    hidden_chunks = wgv.shape[0]

    def gate_copy(c):
        span = pl.ds(c * hidden_chunk, hidden_chunk)
        return pltpu.make_async_copy(wg.at[0, :, span], wgv.at[c], wg_m.at[c])

    def up_copy(c):
        span = pl.ds(c * hidden_chunk, hidden_chunk)
        return pltpu.make_async_copy(wu.at[0, :, span], wuv.at[c], wu_m.at[c])

    def down_copy(c):
        span = pl.ds(c * column_chunk, column_chunk)
        return pltpu.make_async_copy(wd.at[0, :, span], wdv.at[c], wd_m.at[c])

    block = act.shape[0] // row_blocks
    across = model_width // outer

    def part(r):
        return pl.ds(pl.multiple_of(r * block, block), block)

    def begin():
        dense[3].start()
        for c in range(hidden_chunks):
            gate_copy(c).start()
            up_copy(c).start()
        for c in (0, 1, 2, 4):
            dense[c].start()
        for c in range(chunks):
            down_copy(sibling * chunks + c).start()
            down_copy(side * chunks + c).start()
        for sums in (gate_sum, up_sum, dense_gate_sum, dense_up_sum, squares):
            sums[...] = jnp.zeros_like(sums)

    def arrive():
        dense[3].wait()
        dense[0].wait()
        dense[1].wait()
        for c in range(hidden_chunks):
            gate_copy(c).wait()
            up_copy(c).wait()

    turned = (((1,), (1,)), ((), ()))

    def group(plane):
        span = pl.ds(pl.multiple_of(plane * across, across), across)

        def one(r):
            values = res[part(r), span].astype(f32)
            squares[part(r), :] += jnp.sum(values * values, axis=-1, keepdims=True)
            scaled = (values * gain[:, span]).astype(bf16)
            for c in range(hidden_chunks):
                gate_sum[c, part(r), :] += jnp.dot(
                    scaled, wgv[c, span, :], preferred_element_type=f32
                )
                up_sum[c, part(r), :] += jnp.dot(
                    scaled, wuv[c, span, :], preferred_element_type=f32
                )
            dense_gate_sum[part(r), :] += lax.dot_general(
                scaled, dgv[:, span], turned, preferred_element_type=f32
            )
            dense_up_sum[part(r), :] += lax.dot_general(
                scaled, duv[:, span], turned, preferred_element_type=f32
            )

        with jax.named_scope("group"):
            loop(0, row_blocks, one)

    def products():
        received = jnp.broadcast_to(rww[...], (count, sequences, lanes)).reshape(rows, lanes)
        line = lax.broadcasted_iota(jnp.int32, (rows, lanes), 0) % sequences
        lane = lax.broadcasted_iota(jnp.int32, (rows, lanes), 1)
        row_weight[...] = jnp.sum(jnp.where(line == lane, received, 0.0), axis=-1, keepdims=True)

        row_scale = lax.rsqrt(squares[...] / model_width + norm_eps)
        squares[...] = row_scale

        def activate(r):
            scale_rows = squares[part(r), :]
            gate_rows = dense_gate_sum[part(r), :] * scale_rows
            lift_rows = dense_up_sum[part(r), :] * scale_rows
            dense_act[part(r), :] = (gate_rows * sigmoid(gate_rows) * lift_rows).astype(bf16)
            for c in range(hidden_chunks):
                gate_pre = jnp.minimum(gate_sum[c, part(r), :] * scale_rows, clamp_limit)
                up_pre = jnp.clip(up_sum[c, part(r), :] * scale_rows, -clamp_limit, clamp_limit)
                act[part(r), c * hidden_chunk : (c + 1) * hidden_chunk] = (
                    (up_pre + 1.0) * gate_pre * sigmoid(sigmoid_slope * gate_pre)
                ).astype(bf16)

        with jax.named_scope("hidden"):
            loop(0, row_blocks, activate)

        dense[2].wait()
        dense[4].wait()

        def term(c, r):
            span = pl.ds(pl.multiple_of(c * column_chunk, column_chunk), column_chunk)
            routed = jnp.dot(act[part(r), :], wdv[c], preferred_element_type=f32)
            dense_out = jnp.dot(dense_act[part(r), :], ddv[:, span], preferred_element_type=f32)
            return dense_out * scale[:, span] + row_weight[part(r), :] * routed

        def cross(c):
            return remote(passed.at[c], landed.at[c], tp_s, tp_r.at[c], tp=sibling)

        def spread_plane(c, plane):
            def send(t):
                spot = place.spot(t)
                remote(
                    summed.at[c, plane, spot],
                    land1.at[c, plane, n],
                    l1_s,
                    l1_r.at[c * outer + plane],
                    ep=place.at(o, spot),
                ).start()

            loop(1, inner, send)

        def spread(c):
            cross(c).wait_recv()
            both = kept[c] + landed[c].astype(f32)
            summed[c] = both.astype(bf16).reshape(outer, inner, sequences, column_chunk)

            loop(1, outer, lambda t: spread_plane(c, place.plane(t)))

        def give_step(c):
            down_copy(sibling * chunks + c).wait()

            def give(r):
                passed[c, part(r), :] = term(sibling * chunks + c, r).astype(bf16)

            loop(0, row_blocks, give)
            cross(c).start()

        def keep_step(c):
            down_copy(side * chunks + c).wait()

            def keep(r):
                kept[c, part(r), :] = term(side * chunks + c, r)

            loop(0, row_blocks, keep)
            spread(c)

        with jax.named_scope("give"):
            give_step(0)

            def turn(c):
                give_step(c)
                keep_step(c - 1)

            loop(1, chunks, turn)
        with jax.named_scope("keep"):
            keep_step(chunks - 1)

        loop(0, chunks, lambda c: spread_plane(c, o))

        def plane_sum(c, plane):
            others = land1.at[c, plane, pl.ds(0, inner - 1)]
            remote(others, others, l1_s, l1_r.at[c * outer + plane], ep=me).wait_recv()
            total = summed[c, plane, n].astype(f32)
            for t in range(1, inner):
                total += land1[c, plane, place.spot(t)].astype(f32)
            return total

        def first_sum(c):
            def send(t):
                plane = place.plane(t)
                mid[c, plane] = plane_sum(c, plane).astype(bf16)
                remote(
                    mid.at[c, plane], land2.at[c, o], l2_s, l2_r.at[c], ep=place.at(plane, n)
                ).start()

            loop(1, outer, send)

        with jax.named_scope("sum1"):
            loop(0, chunks, first_sum)

        residual = res[
            pl.ds(pl.multiple_of(me * sequences, sequences), sequences),
            pl.ds(pl.multiple_of(side * part_width, part_width), part_width),
        ].astype(f32)

        with jax.named_scope("sum2"):
            for c in range(chunks):
                total = plane_sum(c, o)
                others = land2.at[c, pl.ds(0, outer - 1)]
                remote(others, others, l2_s, l2_r.at[c], ep=me).wait_recv()
                for t in range(1, outer):
                    total += land2[c, place.plane(t)].astype(f32)
                span = slice(c * column_chunk, (c + 1) * column_chunk)
                out[:, span] = (residual[:, span] + total).astype(bf16)

    def settle():
        remote(passed, landed, tp_s, tp_r.at[0], tp=sibling).wait_send()
        others = summed.at[:, :, pl.ds(0, inner - 1)]
        remote(others, others, l1_s, l1_r.at[0], ep=me).wait_send()
        others = mid.at[:, pl.ds(0, outer - 1)]
        remote(others, others, l2_s, l2_r.at[0], ep=me).wait_send()

    def finish():
        products()
        return settle

    return begin, arrive, group, finish


def alone_kernel(outer, inner, *refs):
    first_kernel(outer, inner, *refs)()


def experts_kernel(outer, inner, chunks, row_blocks, *refs):
    place = Place(outer, inner)
    barrier = pltpu.get_barrier_semaphore()
    loop(1, inner, lambda u: greet(barrier, ep=place.at(place.o, place.spot(u))))
    loop(1, outer, lambda t: greet(barrier, ep=place.at(place.plane(t), place.n)))
    greet(barrier, tp=1 - place.side)
    begin, arrive, group, finish = second_kernel(outer, inner, chunks, row_blocks, *refs)
    begin()
    arrive()
    loop(0, outer, group)
    pl.semaphore_wait(barrier, inner + outer - 1)
    finish()()


def whole_kernel(outer, inner, chunks, row_blocks, firsts, *refs):
    first_in, second_in, refs = refs[:15], refs[15:23], refs[23:]
    (mixed, stab_out, mem), (res, rww), refs = refs[:3], refs[3:5], refs[5:]
    begin, arrive, group, finish = second_kernel(
        outer, inner, chunks, row_blocks, res, rww, *second_in, mixed, *refs[firsts:]
    )
    settle = first_kernel(
        outer,
        inner,
        *first_in,
        res,
        rww,
        stab_out,
        mem,
        *refs[:firsts],
        begin=begin,
        ready=arrive,
        group=group,
    )
    finish()()
    settle()


def last_kernel(mixed_in, memory_in, stab_in, mixed, memory, stab, sems):
    pairs = ((memory_in, memory), (mixed_in, mixed), (stab_in, stab))
    moves = [
        pltpu.make_async_copy(source, target, sems.at[i])
        for i, (source, target) in enumerate(pairs)
    ]
    for move in moves:
        move.start()
    for move in moves:
        move.wait()


def in_vmem():
    return pl.BlockSpec(memory_space=pltpu.VMEM)


def in_place():
    return pl.BlockSpec(memory_space=pltpu.HBM)


def held(*arrays):
    return [pltpu.with_memory_space_constraint(array, pltpu.HBM) for array in arrays]


def copies(*numbers):
    return [
        pltpu.SemaphoreType.DMA((number,)) if number else pltpu.SemaphoreType.DMA
        for number in numbers
    ]


def body(
    tokens,
    norm_gain,
    query_weight,
    key_weight,
    value_weight,
    outgate_weight,
    input_weight,
    forget_weight,
    forget_bias,
    memory,
    stabilizer,
    head_gain,
    mix_weight,
    second_gain,
    route_experts,
    route_weight,
    expert_gate,
    expert_up,
    expert_down,
    dense_gate,
    dense_up,
    dense_down,
    branch_scale,
):
    sequences, model_width = tokens.shape
    count = lax.axis_size("ep")
    sides = lax.axis_size("tp")
    inner = 1 << ((count.bit_length() - 1) // 2)
    outer = count // inner
    rows = sequences * count
    half = rows // sides
    width = model_width // count
    heads, size = memory.shape[1], memory.shape[2]
    head_width = query_weight.shape[1]
    part_width = model_width // sides
    topk = route_experts.shape[1]

    aligned = width % lanes == 0
    landing = (sides, half, model_width) if aligned else (count, sides, half, width)
    gates = 2 * heads
    grown = rows // 256

    hidden = expert_gate.shape[2]
    dense_rows = dense_gate.shape[0]
    hidden_chunk = min(hidden, 256)
    column_chunk = min(part_width, 256)
    chunks = part_width // column_chunk
    row_blocks = max(1, grown)
    first_scratch = [
        pltpu.VMEM((sequences, model_width), bf16),
        pltpu.VMEM((1, model_width), f32),
        pltpu.VMEM((heads, width, 4 * size), bf16),
        pltpu.VMEM((heads, width), bf16),
        pltpu.VMEM((heads, width), bf16),
        pltpu.VMEM((1, heads), f32),
        pltpu.VMEM((heads, sequences), f32),
        pltpu.VMEM((heads, size), f32),
        pltpu.VMEM((head_width, width), bf16),
        pltpu.VMEM((topk, sequences), jnp.int32),
        pltpu.VMEM((topk, sequences), f32),
        pltpu.VMEM((count, sequences, width), bf16),
        pltpu.VMEM((count, sequences, width), bf16),
        pltpu.VMEM((count, sequences, width), bf16),
        pltpu.VMEM((count // sides, sequences, width), bf16),
        pltpu.VMEM((count, 1, lanes), f32),
        pltpu.VMEM((outer, inner, sequences, lanes), bf16),
        pltpu.VMEM((inner, outer, sequences, lanes), bf16),
        pltpu.VMEM((outer, sequences, lanes), f32),
        pltpu.VMEM((outer, sequences, lanes), f32),
        pltpu.VMEM((heads, outer, inner, sequences, 4 * size), bf16),
        pltpu.VMEM((heads, outer, inner, sequences, 4 * size), bf16),
        pltpu.VMEM((heads, outer, sequences, 2 * size), f32),
        pltpu.VMEM((heads, outer, sequences, 2 * size), f32),
        pltpu.VMEM((heads, outer, sequences, 2 * size), bf16),
        pltpu.VMEM((heads, outer, sequences, 2 * size), bf16),
        pltpu.VMEM((gates, lanes), f32),
        pltpu.VMEM((heads, sequences, lanes), f32),
        pltpu.VMEM((heads, sequences, lanes), f32),
        pltpu.VMEM((heads, count, sequences, size), bf16),
        pltpu.VMEM((sides, half, width), bf16),
        pltpu.VMEM((half, width), bf16),
    ]
    first_scratch += copies(10, 4 * heads)
    first_scratch += copies(0, 0, 0, count // sides, 0, 0, 0, 0, 0, 0)
    first_scratch += copies(0, heads * outer, 0, heads, 0, heads, heads)
    first_scratch += copies(0, heads, heads, 0, 0, 0, count, 0, outer)
    second_scratch = [
        pltpu.VMEM((1, model_width), f32),
        pltpu.VMEM((1, model_width), f32),
        pltpu.VMEM((hidden // hidden_chunk, model_width, hidden_chunk), bf16),
        pltpu.VMEM((hidden // hidden_chunk, model_width, hidden_chunk), bf16),
        pltpu.VMEM((2 * chunks, hidden, column_chunk), bf16),
        pltpu.VMEM((dense_rows, model_width), bf16),
        pltpu.VMEM((dense_rows, model_width), bf16),
        pltpu.VMEM((dense_rows, model_width), bf16),
        pltpu.VMEM((hidden // hidden_chunk, rows, hidden_chunk), f32),
        pltpu.VMEM((hidden // hidden_chunk, rows, hidden_chunk), f32),
        pltpu.VMEM((rows, dense_rows), f32),
        pltpu.VMEM((rows, dense_rows), f32),
        pltpu.VMEM((rows, 1), f32),
        pltpu.VMEM((rows, dense_rows), bf16),
        pltpu.VMEM((rows, 1), f32),
        pltpu.VMEM((rows, hidden), bf16),
        pltpu.VMEM((chunks, rows, column_chunk), bf16),
        pltpu.VMEM((chunks, rows, column_chunk), bf16),
        pltpu.VMEM((chunks, rows, column_chunk), f32),
        pltpu.VMEM((chunks, outer, inner, sequences, column_chunk), bf16),
        pltpu.VMEM((chunks, outer, inner, sequences, column_chunk), bf16),
        pltpu.VMEM((chunks, outer, sequences, column_chunk), bf16),
        pltpu.VMEM((chunks, outer, sequences, column_chunk), bf16),
    ]
    second_scratch += copies(hidden // hidden_chunk, hidden // hidden_chunk, 2 * chunks, 5)
    second_scratch += copies(0, chunks, 0, chunks * outer, 0, chunks)
    first_arguments = held(
        tokens,
        norm_gain.reshape(1, model_width),
        query_weight,
        key_weight,
        value_weight,
        outgate_weight,
        input_weight.T,
        forget_weight.T,
        forget_bias.reshape(1, heads),
        stabilizer.T,
        head_gain.reshape(heads, size),
        mix_weight,
        route_experts.T,
        route_weight.T,
        memory,
    )
    second_arguments = held(
        second_gain.reshape(1, model_width),
        branch_scale.reshape(1, model_width),
        expert_gate,
        expert_up,
        expert_down,
        dense_gate,
        dense_up,
        dense_down,
    )
    mixed_shape = jax.ShapeDtypeStruct((sequences, part_width), bf16)
    stab_shape = jax.ShapeDtypeStruct((heads, sequences), f32)
    memory_shape = jax.ShapeDtypeStruct(memory.shape, f32)
    if aligned:
        mixed, stab_new, memory_new = pl.pallas_call(
            functools.partial(
                whole_kernel, outer, inner, chunks, row_blocks, len(first_scratch)
            ),
            out_shape=(mixed_shape, stab_shape, memory_shape),
            in_specs=[in_place()] * 23,
            out_specs=(in_vmem(),) * 3,
            scratch_shapes=[
                pltpu.VMEM((rows, model_width), bf16),
                pltpu.VMEM((count, 1, lanes), f32),
            ]
            + first_scratch
            + second_scratch,
            compiler_params=pltpu.CompilerParams(
                collective_id=1, has_side_effects=True, vmem_limit_bytes=44 * 2**20
            ),
        )(*first_arguments, *second_arguments)
    else:
        residual, row_weights, stab_new, memory_new = pl.pallas_call(
            functools.partial(alone_kernel, outer, inner),
            out_shape=(
                jax.ShapeDtypeStruct((count, sides, half, width), bf16),
                jax.ShapeDtypeStruct((count, 1, lanes), f32),
                stab_shape,
                memory_shape,
            ),
            in_specs=[in_place()] * 15,
            out_specs=(in_vmem(),) * 4,
            scratch_shapes=first_scratch,
            compiler_params=pltpu.CompilerParams(
                collective_id=1, has_side_effects=True, vmem_limit_bytes=46 * 2**20
            ),
        )(*first_arguments)
        residual = residual.transpose(1, 2, 0, 3).reshape(rows, model_width)
        mixed = pl.pallas_call(
            functools.partial(experts_kernel, outer, inner, chunks, row_blocks),
            out_shape=mixed_shape,
            in_specs=[in_vmem()] * 2 + [in_place()] * 8,
            out_specs=in_vmem(),
            scratch_shapes=second_scratch,
            compiler_params=pltpu.CompilerParams(
                collective_id=2, has_side_effects=True, vmem_limit_bytes=56 * 2**20
            ),
        )(residual, row_weights, *second_arguments)

    mixed, memory_new, stab_new = pl.pallas_call(
        last_kernel,
        out_shape=tuple(
            jax.ShapeDtypeStruct(array.shape, array.dtype)
            for array in (mixed, memory_new, stab_new)
        ),
        in_specs=[in_vmem()] * 3,
        out_specs=(in_place(),) * 3,
        scratch_shapes=copies(3),
        compiler_params=pltpu.CompilerParams(vmem_limit_bytes=8 * 2**20),
    )(mixed, memory_new, stab_new)
    return (mixed, memory_new, stab_new.T)


def solution(mesh):
    in_specs = (
        P("ep", None),
        P(),
        P("ep", "tp"),
        P("ep", "tp"),
        P("ep", "tp"),
        P("ep", "tp"),
        P("ep", "tp"),
        P("ep", "tp"),
        P("tp"),
        P("ep", "tp", None, None),
        P("ep", "tp"),
        P("tp"),
        P("tp", "ep"),
        P(),
        P("ep", None),
        P("ep", None),
        P("ep", None, "tp"),
        P("ep", None, "tp"),
        P("ep", "tp", None),
        P(("ep", "tp"), None),
        P(("ep", "tp"), None),
        P(("ep", "tp"), None),
        P(),
    )
    out_specs = (P("ep", "tp"), P("ep", "tp", None, None), P("ep", "tp"))
    return jax.shard_map(body, mesh=mesh, in_specs=in_specs, out_specs=out_specs, check_vma=False)
```

```python
import functools

import jax
import jax.numpy as jnp
from jax import lax
from jax.experimental import pallas as pl
from jax.experimental.pallas import tpu as pltpu
from jax.sharding import PartitionSpec as P

norm_eps = 1e-05
clamp_limit = 7.0
sigmoid_slope = 1.702
lanes = 128
f32 = jnp.float32
bf16 = jnp.bfloat16


def loop(lower, upper, step):
    def run(index, carry):
        step(index)
        return carry

    lax.fori_loop(lower, upper, run, 0)


def remote(source, landing, send_sem, recv_sem, **target):
    return pltpu.make_async_remote_copy(
        src_ref=source,
        dst_ref=landing,
        send_sem=send_sem,
        recv_sem=recv_sem,
        device_id=target,
        device_id_type=pl.DeviceIdType.MESH,
    )


def greet(barrier, **target):
    pl.semaphore_signal(
        barrier, inc=1, device_id=target, device_id_type=pl.DeviceIdType.MESH
    )


class Place:
    def __init__(self, outer, inner):
        self.outer, self.inner = outer, inner
        self.me = lax.axis_index("ep")
        self.side = lax.axis_index("tp")
        self.o = self.me // inner
        self.n = self.me % inner

    def plane(self, step):
        return (self.o + step) % self.outer

    def spot(self, step):
        return (self.n + step) % self.inner

    def at(self, plane, spot):
        return plane * self.inner + spot


def gather(place, slot, plane_sem, spot_sem, recv_sem, arrived, complete):
    outer, inner, me = place.outer, place.inner, place.me

    def copy(source, target, send_sem):
        return remote(
            slot(source), slot(source), send_sem, recv_sem.at[source], ep=target
        )

    loop(1, outer, lambda t: copy(me, place.at(place.plane(t), place.n), plane_sem).start())
    loop(1, inner, lambda u: copy(me, place.at(place.o, place.spot(u)), spot_sem).start())
    arrived(me)

    def relay(t):
        source = place.at(place.plane(t), place.n)
        copy(source, source, spot_sem).wait_recv()
        loop(
            1,
            inner,
            lambda u: copy(source, place.at(place.o, place.spot(u)), spot_sem).start(),
        )
        arrived(source)

    loop(1, outer, relay)

    def take(t):
        def one(u):
            source = place.at(place.plane(t), place.spot(u))
            copy(source, source, spot_sem).wait_recv()
            arrived(source)

        loop(1, inner, one)

    take(0)

    def turn(t):
        take(t)
        complete(t - 1)

    loop(1, outer, turn)
    complete(outer - 1)


def sigmoid(values):
    return 1.0 / (1.0 + jnp.exp(-values))


def first_kernel(
    outer,
    inner,
    tok_in,
    norm_gain_in,
    wq,
    wk,
    wv,
    wo,
    wi_in,
    wf_in,
    bias_in,
    stab_in,
    head_gain_in,
    mix_in,
    rexp_in,
    rwt_in,
    mem_in,
    res,
    rww,
    stab_out,
    mem,
    tok,
    norm_gain,
    wide,
    wi,
    wf,
    bias,
    stab,
    hgain,
    mix,
    rexp,
    rwt,
    nbuf,
    nland,
    tbuf,
    tland,
    rbuf,
    pg,
    gland1,
    gmid,
    gland2,
    pbuf,
    land1,
    mid,
    land2,
    mid_half,
    land2_half,
    turned,
    carried_rows,
    written_rows,
    gland,
    pv,
    came,
    mixp,
    in_s,
    wide_s,
    p1_s,
    p1_r,
    tk_s,
    tk_r,
    rt_s,
    rt_r,
    g1_s,
    g1_r,
    g2_s,
    g2_r,
    l1_s,
    l1_r,
    l2_s,
    l2_r,
    l3_s,
    l3_r,
    mi,
    ag_s,
    ag_r,
    ap_r,
    tp_s,
    tp_r,
    ar_s,
    ar_r,
    sb_s,
    sb_r,
    mx_s,
    mx_r,
    ar_p,
    planar=False,
    begin=lambda: None,
    ready=lambda: None,
    group=None,
):
    place = Place(outer, inner)
    me, side, o, n = place.me, place.side, place.o, place.n
    count = outer * inner
    sequences, heads, size = mem.shape[0], mem.shape[1], mem.shape[2]
    width = nland.shape[2]
    rows = count * sequences
    half = rows // 2
    part_spots = inner // 2
    per_half = count // 2
    sibling = 1 - side

    barrier = pltpu.get_barrier_semaphore()
    loop(1, count, lambda t: greet(barrier, ep=(me + t) % count))
    greet(barrier, tp=sibling)
    small = [
        pltpu.make_async_copy(source, target, in_s.at[i])
        for i, (source, target) in enumerate(
            (
                (tok_in, tok),
                (norm_gain_in, norm_gain),
                (rexp_in, rexp),
                (rwt_in, rwt),
                (wi_in, wi),
                (wf_in, wf),
                (bias_in, bias),
                (stab_in, stab),
                (head_gain_in, hgain),
                (mix_in, mix),
            )
        )
    ]
    for copy in small[:6]:
        copy.start()

    def wide_copies(h):
        part = slice(h * size, (h + 1) * size)
        return [
            pltpu.make_async_copy(
                weight.at[:, part],
                wide.at[h, :, slice(j * size, (j + 1) * size)],
                wide_s.at[4 * h + j],
            )
            for j, weight in enumerate((wq, wk, wv, wo))
        ]

    for h in range(heads):
        for copy in wide_copies(h):
            copy.start()
    for copy in small[6:]:
        copy.start()
    loop(
        0,
        heads,
        lambda h: pltpu.make_async_copy(mem_in.at[:, h], mem.at[:, h], mi.at[h]).start(),
    )

    small[0].wait()
    small[1].wait()
    tokens = tok[...].astype(f32)
    mean_square = jnp.mean(tokens * tokens, axis=-1, keepdims=True)
    normed = (tokens * lax.rsqrt(mean_square + norm_eps) * norm_gain[...]).astype(bf16)
    for p in range(count):
        nbuf[p] = normed[:, p * width : (p + 1) * width]

    with jax.named_scope("barrier"):
        pl.semaphore_wait(barrier, count)

    def send_normed(t):
        peer = (me + t) % count
        remote(nbuf.at[peer], nland.at[me], p1_s, p1_r, ep=peer).start()

    loop(1, count, send_normed)
    nland[me] = nbuf[me]

    small[2].wait()
    small[3].wait()
    topk = rexp.shape[0]
    experts = lax.broadcasted_iota(jnp.int32, (count, sequences), 0)
    weights = jnp.zeros((count, sequences), f32)
    for k in range(topk):
        weights += jnp.where(rexp[k : k + 1, :] == experts, rwt[k : k + 1, :], 0.0)
    rbuf[...] = jnp.zeros_like(rbuf)
    for p in range(count):
        rbuf[p, :, :sequences] = weights[p : p + 1, :]

    for p in range(count):
        tbuf[p] = tok[:, p * width : (p + 1) * width]
    begin()
    mine = side == me // per_half

    def token_copy(t):
        peer = (me + t) % count
        return remote(
            tbuf.at[peer], tland.at[me % per_half], tk_s, tk_r.at[me % per_half], ep=peer
        )

    def own_blocks(plane):
        return pl.ds(plane * inner + side * part_spots, part_spots)

    if planar:

        def send_tokens(t):
            plane = place.plane(t)
            remote(
                tbuf.at[own_blocks(plane)],
                tland.at[o],
                tk_s,
                tk_r.at[0],
                ep=place.at(plane, n),
            ).start()

        loop(1, outer, send_tokens)
        tland[o] = tbuf[own_blocks(o)]
    else:

        @pl.when(mine)
        def _():
            loop(1, count, lambda t: token_copy(t).start())
            tland[me % per_half] = tbuf[me]

    def send_route(t):
        peer = (me + t) % count
        remote(rbuf.at[peer], rww.at[me], rt_s, rt_r, ep=peer).start()

    loop(1, count, send_route)
    rww[me] = rbuf[me]

    small[4].wait()
    small[5].wait()
    gates = 2 * heads
    once = jnp.concatenate((wi[...].astype(f32), wf[...].astype(f32)), axis=0)
    thin = jnp.concatenate(
        (once, once, jnp.zeros((lanes - 2 * gates, width), f32)), axis=0
    ).astype(bf16)

    with jax.named_scope("normed"):
        others = nland.at[pl.ds(0, count - 1)]
        remote(others, others, p1_s, p1_r, ep=me).wait_recv()
    columns = nland[...].reshape(rows, width)

    lane = lax.broadcasted_iota(jnp.int32, (rows, lanes), 1)
    thin_sums = lax.dot_general(
        columns, thin, (((1,), (1,)), ((), ())), preferred_element_type=f32
    )
    upper = thin_sums.astype(bf16).astype(f32)
    parted = jnp.where(lane < gates, upper, thin_sums - upper).astype(bf16)
    pg[...] = parted.reshape(outer, inner, sequences, lanes)

    def send_gates(t):
        spot = place.spot(t)
        remote(
            pg.at[:, spot], gland1.at[n], g1_s, g1_r, ep=place.at(o, spot)
        ).start()

    loop(1, inner, send_gates)

    def send_part(h, plane):
        def send(t):
            spot = place.spot(t)
            remote(
                pbuf.at[h, plane, spot],
                land1.at[h, plane, n],
                l1_s,
                l1_r.at[h * outer + plane],
                ep=place.at(o, spot),
            ).start()

        loop(1, inner, send)

    for h in range(heads):
        for copy in wide_copies(h):
            copy.wait()
        sums = jnp.dot(columns, wide[h], preferred_element_type=f32).astype(bf16)
        pbuf[h] = sums.reshape(outer, inner, sequences, 4 * size)
        loop(1, outer, lambda t: send_part(h, place.plane(t)))
        if h > 0:
            send_part(h - 1, o)
    send_part(heads - 1, o)
    for copy in small[6:]:
        copy.wait()

    with jax.named_scope("gates"):
        others = gland1.at[pl.ds(0, inner - 1)]
        remote(others, others, g1_s, g1_r, ep=me).wait_recv()
    for a in range(outer):
        total = pg[a, n].astype(f32)
        for t in range(1, inner):
            total += gland1[place.spot(t), a].astype(f32)
        gmid[a] = total

    def pass_gates(t):
        plane = place.plane(t)
        remote(
            gmid.at[plane], gland2.at[o], g2_s, g2_r, ep=place.at(plane, n)
        ).start()

    loop(1, outer, pass_gates)

    def plane_sum(h, plane):
        with jax.named_scope("first"):
            others = land1.at[h, plane, pl.ds(0, inner - 1)]
            remote(others, others, l1_s, l1_r.at[h * outer + plane], ep=me).wait_recv()
        total = pbuf[h, plane, n].astype(f32)
        for t in range(1, inner):
            total += land1[h, plane, place.spot(t)].astype(f32)
        return total

    def first_sum(h):
        def send(t):
            plane = place.plane(t)
            total = plane_sum(h, plane)
            mid[h, plane] = total[:, : 2 * size]
            mid_half[h, plane] = total[:, 2 * size :].astype(bf16)
            target = place.at(plane, n)
            remote(mid.at[h, plane], land2.at[h, o], l2_s, l2_r.at[h], ep=target).start()
            remote(
                mid_half.at[h, plane], land2_half.at[h, o], l3_s, l3_r.at[h], ep=target
            ).start()

        loop(1, outer, send)

    def gate_math():
        with jax.named_scope("gates2"):
            others = gland2.at[pl.ds(0, outer - 1)]
            remote(others, others, g2_s, g2_r, ep=me).wait_recv()
        total = gmid[o]
        for t in range(1, outer):
            total += gland2[place.plane(t)]
        turn = jnp.transpose(total)
        turn = turn[:gates] + turn[gates : 2 * gates]
        input_pre, forget_pre = turn[:heads], turn[heads:]
        square = lax.broadcasted_iota(jnp.int32, (heads, heads), 0) == lax.broadcasted_iota(
            jnp.int32, (heads, heads), 1
        )
        shift = jnp.sum(jnp.where(square, bias[...], 0.0), axis=1, keepdims=True)
        shifted = forget_pre + shift
        log_forget = jnp.minimum(shifted, 0.0) - jnp.log1p(jnp.exp(-jnp.abs(shifted)))
        stab_new = jnp.maximum(log_forget + stab[...], input_pre)
        stab_out[...] = stab_new
        turned[...] = jnp.zeros_like(turned)
        turned[:heads, :sequences] = jnp.exp(log_forget + stab[...] - stab_new)
        turned[heads:gates, :sequences] = jnp.exp(input_pre - stab_new) * size**-0.5
        back = jnp.transpose(turned[...])[:sequences]
        for h in range(heads):
            carried_rows[h] = jnp.broadcast_to(back[:, h : h + 1], (sequences, lanes))
            written_rows[h] = jnp.broadcast_to(
                back[:, heads + h : heads + h + 1], (sequences, lanes)
            )

    def memory_head(h):
        own = plane_sum(h, o)
        with jax.named_scope("heads"):
            others = land2.at[h, pl.ds(0, outer - 1)]
            remote(others, others, l2_s, l2_r.at[h], ep=me).wait_recv()
            others = land2_half.at[h, pl.ds(0, outer - 1)]
            remote(others, others, l3_s, l3_r.at[h], ep=me).wait_recv()
        pltpu.make_async_copy(mem_in.at[:, h], mem.at[:, h], mi.at[h]).wait()
        query_key, value_gate = own[:, : 2 * size], own[:, 2 * size :]
        for t in range(1, outer):
            query_key += land2[h, place.plane(t)]
            value_gate += land2_half[h, place.plane(t)].astype(f32)
        query_key = query_key.astype(bf16)
        value_gate = value_gate.astype(bf16).astype(f32)
        query, key = query_key[:, :size], query_key[:, size:]
        value, outgate = value_gate[:, :size], value_gate[:, size:]
        value_columns = jnp.transpose(value)
        places = lax.broadcasted_iota(jnp.int32, (size, sequences), 1)
        slots = lax.broadcasted_iota(jnp.int32, (size, lanes), 1)
        query = query.astype(f32)
        carry, write = carried_rows[h], written_rows[h]
        answers = jnp.zeros((size, lanes), f32)
        for s in range(sequences):
            column = jnp.where(places == s, value_columns, 0.0).astype(bf16)
            product = jnp.dot(column, key, preferred_element_type=f32)
            updated = carry[s : s + 1, :] * mem[s, h] + write[s : s + 1, :] * product
            mem[s, h] = updated
            answer = jnp.sum(updated * query[s : s + 1, :], axis=1, keepdims=True)
            answers = jnp.where(slots == s, answer, answers)
        readout = jnp.transpose(answers)[:sequences]
        mean_square = jnp.mean(readout * readout, axis=-1, keepdims=True)
        gated = (
            readout
            * lax.rsqrt(mean_square + norm_eps)
            * hgain[pl.ds(h, 1), :]
            * sigmoid(outgate)
        )
        gland[h, me] = gated.astype(bf16)
        block = gland.at[h, me]
        loop(
            1,
            outer,
            lambda t: remote(
                block, block, ag_s, ag_r.at[h], ep=place.at(place.plane(t), n)
            ).start(),
        )
        if not planar:
            loop(
                1,
                inner,
                lambda u: remote(
                    block, block, ag_s, ap_r.at[h], ep=place.at(o, place.spot(u))
                ).start(),
            )

    def relay(h):
        others = gland.at[h, pl.ds(0, outer - 1)]
        remote(others, others, ag_s, ag_r.at[h], ep=me).wait_recv()

        def one(t):
            block = gland.at[h, place.at(place.plane(t), n)]
            loop(
                1,
                inner,
                lambda u: remote(
                    block, block, ag_s, ap_r.at[h], ep=place.at(o, place.spot(u))
                ).start(),
            )

        loop(1, outer, one)

    def head_step(h):
        @pl.when(h < heads)
        def _():
            first_sum(h)

        @pl.when(h == 0)
        def _():
            gate_math()

        if planar:

            @pl.when(h == heads)
            def _():
                loop(
                    1,
                    inner,
                    lambda u: remote(
                        mix, mixp.at[n], mx_s, mx_r, ep=place.at(o, place.spot(u))
                    ).start(),
                )

        @pl.when(h > 0)
        def _():
            memory_head(h - 1)

    loop(0, heads + 1, head_step)

    def together():
        with jax.named_scope("gated"):
            mixp[n] = mix[...]
            lines = []
            for h in range(heads):
                others = gland.at[h, pl.ds(0, outer - 1)]
                remote(others, others, ag_s, ag_r.at[h], ep=me).wait_recv()
                lines.append(
                    jnp.concatenate([gland[h, place.at(a, n)] for a in range(outer)], axis=0)
                )
            lines = jnp.concatenate(lines, axis=1)
            others = mixp.at[pl.ds(0, inner - 1)]
            remote(others, others, mx_s, mx_r, ep=me).wait_recv()
            for i in range(inner):
                pv[i // part_spots, i % part_spots] = jnp.dot(
                    lines, mixp[i], preferred_element_type=f32
                ).astype(bf16)
        swap = remote(pv.at[sibling], came, tp_s, tp_r, tp=sibling)
        swap.start()
        others = tland.at[pl.ds(0, outer - 1)]
        remote(others, others, tk_s, tk_r.at[0], ep=me).wait_recv()
        with jax.named_scope("swap"):
            swap.wait_recv()
        for i in range(part_spots):
            attended = pv[side, i].astype(f32) + came[i].astype(f32)
            base = (o * inner + side * part_spots + i) * width
            for a in range(outer):
                lower = a * sequences
                res[a, n, :, pl.ds(pl.multiple_of(base, width), width)] = (
                    tland[a, i].astype(f32) + attended[lower : lower + sequences]
                ).astype(bf16)
        return swap

    def apart():
        with jax.named_scope("gated"):
            loop(0, heads, relay)
            partial = jnp.zeros((rows, width), f32)
            for h in range(heads):
                others = gland.at[h, pl.ds(0, outer * (inner - 1))]
                remote(others, others, ag_s, ap_r.at[h], ep=me).wait_recv()
                partial += jnp.dot(
                    gland[h].reshape(rows, size),
                    mix[h * size : (h + 1) * size, :],
                    preferred_element_type=f32,
                )
            partial = partial.astype(bf16)
        pv[...] = partial.reshape(2, half, width)
        swap = remote(pv.at[sibling], came, tp_s, tp_r, tp=sibling)
        swap.start()

        def take_tokens(b):
            source = side * per_half + b

            @pl.when(source != me)
            def _():
                remote(tland.at[b], tland.at[b], tk_s, tk_r.at[b], ep=source).wait_recv()

        loop(0, per_half, take_tokens)
        with jax.named_scope("swap"):
            swap.wait_recv()
        attended = pv[side].astype(f32) + came[...].astype(f32)
        residual = (tland[...].reshape(half, width).astype(f32) + attended).astype(bf16)
        res[me, side] = residual
        return swap

    swap = together() if planar else apart()

    def slot(p, core):
        if planar:
            base = (p // inner * inner + core * part_spots) * width
            return res.at[
                :, p % inner, :, pl.ds(pl.multiple_of(base, width), part_spots * width)
            ]
        return res.at[p, core]

    def hand(p):
        remote(slot(p, side), slot(p, side), sb_s, sb_r.at[p // inner], tp=sibling).start()

    def complete(t):
        plane = place.plane(t)
        if planar:
            base = (plane * inner + sibling * part_spots) * width
            whole = res.at[:, :, :, pl.ds(pl.multiple_of(base, width), part_spots * width)]
        else:
            whole = res.at[pl.ds(plane * inner, inner), sibling]
        with jax.named_scope("settle"):
            remote(whole, whole, sb_s, sb_r.at[plane], tp=sibling).wait_recv()
        if group is not None:
            group(plane)

    ready()
    others = rww.at[pl.ds(0, count - 1)]
    remote(others, others, rt_s, rt_r, ep=me).wait()
    with jax.named_scope("rows"):
        gather(place, lambda p: slot(p, side), ar_s, ar_p, ar_r, hand, complete)

    def settle():
        if planar:
            block = part_spots * width
            whole = res.at[:, :, :, pl.ds(0, outer * block)]
            sent = res.at[:, pl.ds(0, outer - 1), :, pl.ds(0, block)]
            passed = res.at[:, pl.ds(0, inner - 1), :, pl.ds(0, outer * block)]
        else:
            whole, sent = res.at[:, side], res.at[pl.ds(0, outer - 1), side]
            passed = res.at[pl.ds(0, outer * (inner - 1)), side]
        remote(whole, whole, sb_s, sb_r.at[0], tp=sibling).wait_send()
        remote(sent, sent, ar_s, ar_r.at[0], ep=me).wait_send()
        remote(passed, passed, ar_p, ar_r.at[0], ep=me).wait_send()
        others = nbuf.at[pl.ds(0, count - 1)]
        remote(others, others, p1_s, p1_r, ep=me).wait_send()

        if planar:
            others = tland.at[pl.ds(0, outer - 1)]
            remote(others, others, tk_s, tk_r.at[0], ep=me).wait_send()
            others = mixp.at[pl.ds(0, inner - 1)]
            remote(others, others, mx_s, mx_r, ep=me).wait_send()
        else:

            @pl.when(mine)
            def _():
                remote(others, others, tk_s, tk_r.at[0], ep=me).wait_send()

        others = gland1.at[pl.ds(0, inner - 1)]
        remote(others, others, g1_s, g1_r, ep=me).wait_send()
        others = gmid.at[pl.ds(0, outer - 1)]
        remote(others, others, g2_s, g2_r, ep=me).wait_send()
        others = pbuf.at[:, :, pl.ds(0, inner - 1)]
        remote(others, others, l1_s, l1_r.at[0], ep=me).wait_send()
        others = mid.at[:, pl.ds(0, outer - 1)]
        remote(others, others, l2_s, l2_r.at[0], ep=me).wait_send()
        others = mid_half.at[:, pl.ds(0, outer - 1)]
        remote(others, others, l3_s, l3_r.at[0], ep=me).wait_send()
        others = gland.at[:, pl.ds(0, (outer if planar else count) - 1)]
        remote(others, others, ag_s, ag_r.at[0], ep=me).wait_send()
        swap.wait_send()

    return settle


def second_kernel(
    outer,
    inner,
    chunks,
    row_blocks,
    res,
    rww,
    gain_in,
    scale_in,
    wg,
    wu,
    wd,
    dg,
    du,
    dd,
    out,
    gain,
    scale,
    wgv,
    wuv,
    wdv,
    dgv,
    duv,
    ddv,
    gate_sum,
    up_sum,
    dense_gate_sum,
    dense_up_sum,
    squares,
    dense_act,
    row_weight,
    act,
    passed,
    landed,
    kept,
    summed,
    land1,
    mid,
    land2,
    wg_m,
    wu_m,
    wd_m,
    d_m,
    tp_s,
    tp_r,
    l1_s,
    l1_r,
    l2_s,
    l2_r,
):
    place = Place(outer, inner)
    me, side, o, n = place.me, place.side, place.o, place.n
    count = outer * inner
    rows, model_width = act.shape[0], res.shape[-1]
    sequences = rows // count
    sibling = 1 - side
    hidden_chunk = wgv.shape[2]
    column_chunk = wdv.shape[2]
    part_width = chunks * column_chunk

    dense = [
        pltpu.make_async_copy(source, target, d_m.at[i])
        for i, (source, target) in enumerate(
            ((dg, dgv), (du, duv), (dd, ddv), (gain_in, gain), (scale_in, scale))
        )
    ]
    hidden_chunks = wgv.shape[0]

    def gate_copy(c):
        span = pl.ds(c * hidden_chunk, hidden_chunk)
        return pltpu.make_async_copy(wg.at[0, :, span], wgv.at[c], wg_m.at[c])

    def up_copy(c):
        span = pl.ds(c * hidden_chunk, hidden_chunk)
        return pltpu.make_async_copy(wu.at[0, :, span], wuv.at[c], wu_m.at[c])

    def down_copy(c):
        span = pl.ds(c * column_chunk, column_chunk)
        return pltpu.make_async_copy(wd.at[0, :, span], wdv.at[c], wd_m.at[c])

    block = act.shape[0] // row_blocks
    across = model_width // outer

    def part(r):
        return pl.ds(pl.multiple_of(r * block, block), block)

    def begin():
        dense[3].start()
        for c in range(hidden_chunks):
            gate_copy(c).start()
            up_copy(c).start()
        for c in (0, 1, 2, 4):
            dense[c].start()
        for c in range(chunks):
            down_copy(sibling * chunks + c).start()
            down_copy(side * chunks + c).start()
        for sums in (gate_sum, up_sum, dense_gate_sum, dense_up_sum, squares):
            sums[...] = jnp.zeros_like(sums)

    def arrive():
        dense[3].wait()
        dense[0].wait()
        dense[1].wait()
        for c in range(hidden_chunks):
            gate_copy(c).wait()
            up_copy(c).wait()

    turned = (((1,), (1,)), ((), ()))

    def group(plane):
        span = pl.ds(pl.multiple_of(plane * across, across), across)

        def one(r):
            if len(res.shape) == 4:
                values = res[:, :, :, span].reshape(rows, across).astype(f32)
            else:
                values = res[part(r), span].astype(f32)
            squares[part(r), :] += jnp.sum(values * values, axis=-1, keepdims=True)
            scaled = (values * gain[:, span]).astype(bf16)
            for c in range(hidden_chunks):
                gate_sum[c, part(r), :] += jnp.dot(
                    scaled, wgv[c, span, :], preferred_element_type=f32
                )
                up_sum[c, part(r), :] += jnp.dot(
                    scaled, wuv[c, span, :], preferred_element_type=f32
                )
            dense_gate_sum[part(r), :] += lax.dot_general(
                scaled, dgv[:, span], turned, preferred_element_type=f32
            )
            dense_up_sum[part(r), :] += lax.dot_general(
                scaled, duv[:, span], turned, preferred_element_type=f32
            )

        with jax.named_scope("group"):
            loop(0, row_blocks, one)

    def products():
        received = jnp.broadcast_to(rww[...], (count, sequences, lanes)).reshape(rows, lanes)
        line = lax.broadcasted_iota(jnp.int32, (rows, lanes), 0) % sequences
        lane = lax.broadcasted_iota(jnp.int32, (rows, lanes), 1)
        row_weight[...] = jnp.sum(jnp.where(line == lane, received, 0.0), axis=-1, keepdims=True)

        row_scale = lax.rsqrt(squares[...] / model_width + norm_eps)
        squares[...] = row_scale

        def activate(r):
            scale_rows = squares[part(r), :]
            gate_rows = dense_gate_sum[part(r), :] * scale_rows
            lift_rows = dense_up_sum[part(r), :] * scale_rows
            dense_act[part(r), :] = (gate_rows * sigmoid(gate_rows) * lift_rows).astype(bf16)
            for c in range(hidden_chunks):
                gate_pre = jnp.minimum(gate_sum[c, part(r), :] * scale_rows, clamp_limit)
                up_pre = jnp.clip(up_sum[c, part(r), :] * scale_rows, -clamp_limit, clamp_limit)
                act[part(r), c * hidden_chunk : (c + 1) * hidden_chunk] = (
                    (up_pre + 1.0) * gate_pre * sigmoid(sigmoid_slope * gate_pre)
                ).astype(bf16)

        with jax.named_scope("hidden"):
            loop(0, row_blocks, activate)

        dense[2].wait()
        dense[4].wait()

        def term(c, r):
            span = pl.ds(pl.multiple_of(c * column_chunk, column_chunk), column_chunk)
            routed = jnp.dot(act[part(r), :], wdv[c], preferred_element_type=f32)
            dense_out = jnp.dot(dense_act[part(r), :], ddv[:, span], preferred_element_type=f32)
            return dense_out * scale[:, span] + row_weight[part(r), :] * routed

        def cross(c):
            return remote(passed.at[c], landed.at[c], tp_s, tp_r.at[c], tp=sibling)

        def spread_plane(c, plane):
            def send(t):
                spot = place.spot(t)
                remote(
                    summed.at[c, plane, spot],
                    land1.at[c, plane, n],
                    l1_s,
                    l1_r.at[c * outer + plane],
                    ep=place.at(o, spot),
                ).start()

            loop(1, inner, send)

        def spread(c):
            cross(c).wait_recv()
            both = kept[c] + landed[c].astype(f32)
            summed[c] = both.astype(bf16).reshape(outer, inner, sequences, column_chunk)

            loop(1, outer, lambda t: spread_plane(c, place.plane(t)))

        def give_step(c):
            down_copy(sibling * chunks + c).wait()

            def give(r):
                passed[c, part(r), :] = term(sibling * chunks + c, r).astype(bf16)

            loop(0, row_blocks, give)
            cross(c).start()

        def keep_step(c):
            down_copy(side * chunks + c).wait()

            def keep(r):
                kept[c, part(r), :] = term(side * chunks + c, r)

            loop(0, row_blocks, keep)
            spread(c)

        with jax.named_scope("give"):
            give_step(0)

            def turn(c):
                give_step(c)
                keep_step(c - 1)

            loop(1, chunks, turn)
        with jax.named_scope("keep"):
            keep_step(chunks - 1)

        loop(0, chunks, lambda c: spread_plane(c, o))

        def plane_sum(c, plane):
            others = land1.at[c, plane, pl.ds(0, inner - 1)]
            remote(others, others, l1_s, l1_r.at[c * outer + plane], ep=me).wait_recv()
            total = summed[c, plane, n].astype(f32)
            for t in range(1, inner):
                total += land1[c, plane, place.spot(t)].astype(f32)
            return total

        def first_sum(c):
            def send(t):
                plane = place.plane(t)
                mid[c, plane] = plane_sum(c, plane).astype(bf16)
                remote(
                    mid.at[c, plane], land2.at[c, o], l2_s, l2_r.at[c], ep=place.at(plane, n)
                ).start()

            loop(1, outer, send)

        with jax.named_scope("sum1"):
            loop(0, chunks, first_sum)

        columns = pl.ds(pl.multiple_of(side * part_width, part_width), part_width)
        if len(res.shape) == 4:
            residual = res[o, n, :, columns].astype(f32)
        else:
            own_rows = pl.ds(pl.multiple_of(me * sequences, sequences), sequences)
            residual = res[own_rows, columns].astype(f32)

        with jax.named_scope("sum2"):
            for c in range(chunks):
                total = plane_sum(c, o)
                others = land2.at[c, pl.ds(0, outer - 1)]
                remote(others, others, l2_s, l2_r.at[c], ep=me).wait_recv()
                for t in range(1, outer):
                    total += land2[c, place.plane(t)].astype(f32)
                span = slice(c * column_chunk, (c + 1) * column_chunk)
                out[:, span] = (residual[:, span] + total).astype(bf16)

    def settle():
        remote(passed, landed, tp_s, tp_r.at[0], tp=sibling).wait_send()
        others = summed.at[:, :, pl.ds(0, inner - 1)]
        remote(others, others, l1_s, l1_r.at[0], ep=me).wait_send()
        others = mid.at[:, pl.ds(0, outer - 1)]
        remote(others, others, l2_s, l2_r.at[0], ep=me).wait_send()

    def finish():
        products()
        return settle

    return begin, arrive, group, finish


def alone_kernel(outer, inner, *refs):
    first_kernel(outer, inner, *refs)()


def experts_kernel(outer, inner, chunks, row_blocks, *refs):
    place = Place(outer, inner)
    barrier = pltpu.get_barrier_semaphore()
    loop(1, inner, lambda u: greet(barrier, ep=place.at(place.o, place.spot(u))))
    loop(1, outer, lambda t: greet(barrier, ep=place.at(place.plane(t), place.n)))
    greet(barrier, tp=1 - place.side)
    begin, arrive, group, finish = second_kernel(outer, inner, chunks, row_blocks, *refs)
    begin()
    arrive()
    loop(0, outer, group)
    pl.semaphore_wait(barrier, inner + outer - 1)
    finish()()


def whole_kernel(outer, inner, chunks, row_blocks, firsts, *refs):
    first_in, second_in, refs = refs[:15], refs[15:23], refs[23:]
    (mixed, stab_out, mem), (res, rww), refs = refs[:3], refs[3:5], refs[5:]
    begin, arrive, group, finish = second_kernel(
        outer, inner, chunks, row_blocks, res, rww, *second_in, mixed, *refs[firsts:]
    )
    settle = first_kernel(
        outer,
        inner,
        *first_in,
        res,
        rww,
        stab_out,
        mem,
        *refs[:firsts],
        planar=True,
        begin=begin,
        ready=arrive,
        group=group,
    )
    finish()()
    settle()


def last_kernel(mixed_in, memory_in, stab_in, mixed, memory, stab, sems):
    parts = sems.shape[0] - 2
    each = memory.shape[0] // parts
    pairs = [(mixed_in, mixed), (stab_in, stab)]
    for part in range(parts):
        span = pl.ds(part * each, each)
        pairs.append((memory_in.at[span], memory.at[span]))
    moves = [
        pltpu.make_async_copy(source, target, sems.at[i])
        for i, (source, target) in enumerate(pairs)
    ]
    for move in moves:
        move.start()
    for move in moves:
        move.wait()


def in_vmem():
    return pl.BlockSpec(memory_space=pltpu.VMEM)


def in_place():
    return pl.BlockSpec(memory_space=pltpu.HBM)


def held(*arrays):
    return [pltpu.with_memory_space_constraint(array, pltpu.HBM) for array in arrays]


def copies(*numbers):
    return [
        pltpu.SemaphoreType.DMA((number,)) if number else pltpu.SemaphoreType.DMA
        for number in numbers
    ]


def body(
    tokens,
    norm_gain,
    query_weight,
    key_weight,
    value_weight,
    outgate_weight,
    input_weight,
    forget_weight,
    forget_bias,
    memory,
    stabilizer,
    head_gain,
    mix_weight,
    second_gain,
    route_experts,
    route_weight,
    expert_gate,
    expert_up,
    expert_down,
    dense_gate,
    dense_up,
    dense_down,
    branch_scale,
):
    sequences, model_width = tokens.shape
    count = lax.axis_size("ep")
    sides = lax.axis_size("tp")
    inner = 1 << ((count.bit_length() - 1) // 2)
    outer = count // inner
    rows = sequences * count
    half = rows // sides
    width = model_width // count
    heads, size = memory.shape[1], memory.shape[2]
    head_width = query_weight.shape[1]
    part_width = model_width // sides
    topk = route_experts.shape[1]

    aligned = width % lanes == 0
    landing = (sides, half, model_width) if aligned else (count, sides, half, width)
    gates = 2 * heads
    grown = rows // 256

    hidden = expert_gate.shape[2]
    dense_rows = dense_gate.shape[0]
    hidden_chunk = min(hidden, 256)
    column_chunk = min(part_width, 256)
    chunks = part_width // column_chunk
    row_blocks = 1 if aligned else max(1, grown)
    token_landing = (count // sides, sequences, width)
    part_shape = (half, width)
    if aligned:
        token_landing = (outer, inner // sides, sequences, width)
        part_shape = (inner // sides, outer * sequences, width)
    first_scratch = [
        pltpu.VMEM((sequences, model_width), bf16),
        pltpu.VMEM((1, model_width), f32),
        pltpu.VMEM((heads, width, 4 * size), bf16),
        pltpu.VMEM((heads, width), bf16),
        pltpu.VMEM((heads, width), bf16),
        pltpu.VMEM((1, heads), f32),
        pltpu.VMEM((heads, sequences), f32),
        pltpu.VMEM((heads, size), f32),
        pltpu.VMEM((head_width, width), bf16),
        pltpu.VMEM((topk, sequences), jnp.int32),
        pltpu.VMEM((topk, sequences), f32),
        pltpu.VMEM((count, sequences, width), bf16),
        pltpu.VMEM((count, sequences, width), bf16),
        pltpu.VMEM((count, sequences, width), bf16),
        pltpu.VMEM(token_landing, bf16),
        pltpu.VMEM((count, 1, lanes), f32),
        pltpu.VMEM((outer, inner, sequences, lanes), bf16),
        pltpu.VMEM((inner, outer, sequences, lanes), bf16),
        pltpu.VMEM((outer, sequences, lanes), f32),
        pltpu.VMEM((outer, sequences, lanes), f32),
        pltpu.VMEM((heads, outer, inner, sequences, 4 * size), bf16),
        pltpu.VMEM((heads, outer, inner, sequences, 4 * size), bf16),
        pltpu.VMEM((heads, outer, sequences, 2 * size), f32),
        pltpu.VMEM((heads, outer, sequences, 2 * size), f32),
        pltpu.VMEM((heads, outer, sequences, 2 * size), bf16),
        pltpu.VMEM((heads, outer, sequences, 2 * size), bf16),
        pltpu.VMEM((gates, lanes), f32),
        pltpu.VMEM((heads, sequences, lanes), f32),
        pltpu.VMEM((heads, sequences, lanes), f32),
        pltpu.VMEM((heads, count, sequences, size), bf16),
        pltpu.VMEM((sides,) + part_shape, bf16),
        pltpu.VMEM(part_shape, bf16),
        pltpu.VMEM((inner, head_width, width), bf16),
    ]
    first_scratch += copies(10, 4 * heads)
    first_scratch += copies(0, 0, 0, count // sides, 0, 0, 0, 0, 0, 0)
    first_scratch += copies(0, heads * outer, 0, heads, 0, heads, heads)
    first_scratch += copies(0, heads, heads, 0, 0, 0, count, 0, outer, 0, 0, 0)
    second_scratch = [
        pltpu.VMEM((1, model_width), f32),
        pltpu.VMEM((1, model_width), f32),
        pltpu.VMEM((hidden // hidden_chunk, model_width, hidden_chunk), bf16),
        pltpu.VMEM((hidden // hidden_chunk, model_width, hidden_chunk), bf16),
        pltpu.VMEM((2 * chunks, hidden, column_chunk), bf16),
        pltpu.VMEM((dense_rows, model_width), bf16),
        pltpu.VMEM((dense_rows, model_width), bf16),
        pltpu.VMEM((dense_rows, model_width), bf16),
        pltpu.VMEM((hidden // hidden_chunk, rows, hidden_chunk), f32),
        pltpu.VMEM((hidden // hidden_chunk, rows, hidden_chunk), f32),
        pltpu.VMEM((rows, dense_rows), f32),
        pltpu.VMEM((rows, dense_rows), f32),
        pltpu.VMEM((rows, 1), f32),
        pltpu.VMEM((rows, dense_rows), bf16),
        pltpu.VMEM((rows, 1), f32),
        pltpu.VMEM((rows, hidden), bf16),
        pltpu.VMEM((chunks, rows, column_chunk), bf16),
        pltpu.VMEM((chunks, rows, column_chunk), bf16),
        pltpu.VMEM((chunks, rows, column_chunk), f32),
        pltpu.VMEM((chunks, outer, inner, sequences, column_chunk), bf16),
        pltpu.VMEM((chunks, outer, inner, sequences, column_chunk), bf16),
        pltpu.VMEM((chunks, outer, sequences, column_chunk), bf16),
        pltpu.VMEM((chunks, outer, sequences, column_chunk), bf16),
    ]
    second_scratch += copies(hidden // hidden_chunk, hidden // hidden_chunk, 2 * chunks, 5)
    second_scratch += copies(0, chunks, 0, chunks * outer, 0, chunks)
    first_arguments = held(
        tokens,
        norm_gain.reshape(1, model_width),
        query_weight,
        key_weight,
        value_weight,
        outgate_weight,
        input_weight.T,
        forget_weight.T,
        forget_bias.reshape(1, heads),
        stabilizer.T,
        head_gain.reshape(heads, size),
        mix_weight,
        route_experts.T,
        route_weight.T,
        memory,
    )
    second_arguments = held(
        second_gain.reshape(1, model_width),
        branch_scale.reshape(1, model_width),
        expert_gate,
        expert_up,
        expert_down,
        dense_gate,
        dense_up,
        dense_down,
    )
    mixed_shape = jax.ShapeDtypeStruct((sequences, part_width), bf16)
    stab_shape = jax.ShapeDtypeStruct((heads, sequences), f32)
    memory_shape = jax.ShapeDtypeStruct(memory.shape, f32)
    if aligned:
        mixed, stab_new, memory_new = pl.pallas_call(
            functools.partial(
                whole_kernel, outer, inner, chunks, row_blocks, len(first_scratch)
            ),
            out_shape=(mixed_shape, stab_shape, memory_shape),
            in_specs=[in_place()] * 23,
            out_specs=(in_vmem(),) * 3,
            scratch_shapes=[
                pltpu.VMEM((outer, inner, sequences, model_width), bf16),
                pltpu.VMEM((count, 1, lanes), f32),
            ]
            + first_scratch
            + second_scratch,
            compiler_params=pltpu.CompilerParams(
                collective_id=1, has_side_effects=True, vmem_limit_bytes=44 * 2**20
            ),
        )(*first_arguments, *second_arguments)
    else:
        residual, row_weights, stab_new, memory_new = pl.pallas_call(
            functools.partial(alone_kernel, outer, inner),
            out_shape=(
                jax.ShapeDtypeStruct((count, sides, half, width), bf16),
                jax.ShapeDtypeStruct((count, 1, lanes), f32),
                stab_shape,
                memory_shape,
            ),
            in_specs=[in_place()] * 15,
            out_specs=(in_vmem(),) * 4,
            scratch_shapes=first_scratch,
            compiler_params=pltpu.CompilerParams(
                collective_id=1, has_side_effects=True, vmem_limit_bytes=46 * 2**20
            ),
        )(*first_arguments)
        residual = residual.transpose(1, 2, 0, 3).reshape(rows, model_width)
        mixed = pl.pallas_call(
            functools.partial(experts_kernel, outer, inner, chunks, row_blocks),
            out_shape=mixed_shape,
            in_specs=[in_vmem()] * 2 + [in_place()] * 8,
            out_specs=in_vmem(),
            scratch_shapes=second_scratch,
            compiler_params=pltpu.CompilerParams(
                collective_id=2, has_side_effects=True, vmem_limit_bytes=56 * 2**20
            ),
        )(residual, row_weights, *second_arguments)

    mixed, memory_new, stab_new = pl.pallas_call(
        last_kernel,
        out_shape=tuple(
            jax.ShapeDtypeStruct(array.shape, array.dtype)
            for array in (mixed, memory_new, stab_new)
        ),
        in_specs=[in_vmem()] * 3,
        out_specs=(in_place(),) * 3,
        scratch_shapes=copies(2 + min(sequences, 8)),
        compiler_params=pltpu.CompilerParams(vmem_limit_bytes=8 * 2**20),
    )(mixed, memory_new, stab_new)
    return (mixed, memory_new, stab_new.T)


def solution(mesh):
    in_specs = (
        P("ep", None),
        P(),
        P("ep", "tp"),
        P("ep", "tp"),
        P("ep", "tp"),
        P("ep", "tp"),
        P("ep", "tp"),
        P("ep", "tp"),
        P("tp"),
        P("ep", "tp", None, None),
        P("ep", "tp"),
        P("tp"),
        P("tp", "ep"),
        P(),
        P("ep", None),
        P("ep", None),
        P("ep", None, "tp"),
        P("ep", None, "tp"),
        P("ep", "tp", None),
        P(("ep", "tp"), None),
        P(("ep", "tp"), None),
        P(("ep", "tp"), None),
        P(),
    )
    out_specs = (P("ep", "tp"), P("ep", "tp", None, None), P("ep", "tp"))
    return jax.shard_map(body, mesh=mesh, in_specs=in_specs, out_specs=out_specs, check_vma=False)
```

```python
import functools

import jax
import jax.numpy as jnp
from jax import lax
from jax.experimental import pallas as pl
from jax.experimental.pallas import tpu as pltpu
from jax.sharding import PartitionSpec as P

norm_eps = 1e-05
clamp_limit = 7.0
sigmoid_slope = 1.702
lanes = 128
f32 = jnp.float32
bf16 = jnp.bfloat16


def loop(lower, upper, step):
    def run(index, carry):
        step(index)
        return carry

    lax.fori_loop(lower, upper, run, 0)


def remote(source, landing, send_sem, recv_sem, **target):
    return pltpu.make_async_remote_copy(
        src_ref=source,
        dst_ref=landing,
        send_sem=send_sem,
        recv_sem=recv_sem,
        device_id=target,
        device_id_type=pl.DeviceIdType.MESH,
    )


def greet(barrier, **target):
    pl.semaphore_signal(
        barrier, inc=1, device_id=target, device_id_type=pl.DeviceIdType.MESH
    )


class Place:
    def __init__(self, outer, inner):
        self.outer, self.inner = outer, inner
        self.me = lax.axis_index("ep")
        self.side = lax.axis_index("tp")
        self.o = self.me // inner
        self.n = self.me % inner

    def plane(self, step):
        turn = 1 - 2 * (2 * self.o // self.outer)
        return (self.o + turn * step + self.outer) % self.outer

    def spot(self, step):
        return (self.n + step) % self.inner

    def at(self, plane, spot):
        return plane * self.inner + spot


def gather(place, slot, plane_sem, spot_sem, recv_sem, arrived, complete):
    outer, inner, me = place.outer, place.inner, place.me

    def copy(source, target, send_sem):
        return remote(
            slot(source), slot(source), send_sem, recv_sem.at[source], ep=target
        )

    loop(1, outer, lambda t: copy(me, place.at(place.plane(t), place.n), plane_sem).start())
    loop(1, inner, lambda u: copy(me, place.at(place.o, place.spot(u)), spot_sem).start())
    arrived(me)

    def relay(t):
        source = place.at(place.plane(t), place.n)
        copy(source, source, spot_sem).wait_recv()
        loop(
            1,
            inner,
            lambda u: copy(source, place.at(place.o, place.spot(u)), spot_sem).start(),
        )
        arrived(source)

    loop(1, outer, relay)

    def take(t):
        def one(u):
            source = place.at(place.plane(t), place.spot(u))
            copy(source, source, spot_sem).wait_recv()
            arrived(source)

        loop(1, inner, one)

    take(0)

    def turn(t):
        take(t)
        complete(t - 1)

    loop(1, outer, turn)
    complete(outer - 1)


def sigmoid(values):
    return 1.0 / (1.0 + jnp.exp(-values))


def first_kernel(
    outer,
    inner,
    tok_in,
    norm_gain_in,
    wq,
    wk,
    wv,
    wo,
    wi_in,
    wf_in,
    bias_in,
    stab_in,
    head_gain_in,
    mix_in,
    rexp_in,
    rwt_in,
    mem_in,
    res,
    rww,
    stab_out,
    mem,
    tok,
    norm_gain,
    wide,
    wi,
    wf,
    bias,
    stab,
    hgain,
    mix,
    rexp,
    rwt,
    nbuf,
    nland,
    tbuf,
    tland,
    rbuf,
    pg,
    gland1,
    gmid,
    gland2,
    pbuf,
    land1,
    mid,
    land2,
    mid_half,
    land2_half,
    turned,
    carried_rows,
    written_rows,
    gland,
    pv,
    came,
    mixp,
    in_s,
    wide_s,
    p1_s,
    p1_r,
    tk_s,
    tk_r,
    rt_s,
    rt_r,
    g1_s,
    g1_r,
    g2_s,
    g2_r,
    l1_s,
    l1_r,
    l2_s,
    l2_r,
    l3_s,
    l3_r,
    mi,
    ag_s,
    ag_r,
    ap_r,
    tp_s,
    tp_r,
    ar_s,
    ar_r,
    sb_s,
    sb_r,
    mx_s,
    mx_r,
    ar_p,
    planar=False,
    begin=lambda: None,
    ready=lambda: None,
    group=None,
):
    place = Place(outer, inner)
    me, side, o, n = place.me, place.side, place.o, place.n
    count = outer * inner
    sequences, heads, size = mem.shape[0], mem.shape[1], mem.shape[2]
    width = nland.shape[2]
    rows = count * sequences
    half = rows // 2
    part_spots = inner // 2
    per_half = count // 2
    sibling = 1 - side

    barrier = pltpu.get_barrier_semaphore()
    loop(1, count, lambda t: greet(barrier, ep=(me + t) % count))
    greet(barrier, tp=sibling)
    small = [
        pltpu.make_async_copy(source, target, in_s.at[i])
        for i, (source, target) in enumerate(
            (
                (tok_in, tok),
                (norm_gain_in, norm_gain),
                (rexp_in, rexp),
                (rwt_in, rwt),
                (wi_in, wi),
                (wf_in, wf),
                (bias_in, bias),
                (stab_in, stab),
                (head_gain_in, hgain),
                (mix_in, mix),
            )
        )
    ]
    for copy in small[:6]:
        copy.start()

    def wide_copies(h):
        part = slice(h * size, (h + 1) * size)
        return [
            pltpu.make_async_copy(
                weight.at[:, part],
                wide.at[h, :, slice(j * size, (j + 1) * size)],
                wide_s.at[4 * h + j],
            )
            for j, weight in enumerate((wq, wk, wv, wo))
        ]

    for h in range(heads):
        for copy in wide_copies(h):
            copy.start()
    for copy in small[6:]:
        copy.start()
    loop(
        0,
        heads,
        lambda h: pltpu.make_async_copy(mem_in.at[:, h], mem.at[:, h], mi.at[h]).start(),
    )

    small[0].wait()
    small[1].wait()
    tokens = tok[...].astype(f32)
    mean_square = jnp.mean(tokens * tokens, axis=-1, keepdims=True)
    normed = (tokens * lax.rsqrt(mean_square + norm_eps) * norm_gain[...]).astype(bf16)
    for p in range(count):
        nbuf[p] = normed[:, p * width : (p + 1) * width]

    with jax.named_scope("barrier"):
        pl.semaphore_wait(barrier, count)

    def send_normed(t):
        peer = (me + t) % count
        remote(nbuf.at[peer], nland.at[me], p1_s, p1_r, ep=peer).start()

    loop(1, count, send_normed)
    nland[me] = nbuf[me]

    small[2].wait()
    small[3].wait()
    topk = rexp.shape[0]
    experts = lax.broadcasted_iota(jnp.int32, (count, sequences), 0)
    weights = jnp.zeros((count, sequences), f32)
    for k in range(topk):
        weights += jnp.where(rexp[k : k + 1, :] == experts, rwt[k : k + 1, :], 0.0)
    rbuf[...] = jnp.zeros_like(rbuf)
    for p in range(count):
        rbuf[p, :, :sequences] = weights[p : p + 1, :]

    for p in range(count):
        tbuf[p] = tok[:, p * width : (p + 1) * width]
    begin()
    mine = side == me // per_half

    def token_copy(t):
        peer = (me + t) % count
        return remote(
            tbuf.at[peer], tland.at[me % per_half], tk_s, tk_r.at[me % per_half], ep=peer
        )

    def own_blocks(plane):
        return pl.ds(plane * inner + side * part_spots, part_spots)

    if planar:

        def send_tokens(t):
            plane = place.plane(t)
            remote(
                tbuf.at[own_blocks(plane)],
                tland.at[o],
                tk_s,
                tk_r.at[0],
                ep=place.at(plane, n),
            ).start()

        loop(1, outer, send_tokens)
        tland[o] = tbuf[own_blocks(o)]
    else:

        @pl.when(mine)
        def _():
            loop(1, count, lambda t: token_copy(t).start())
            tland[me % per_half] = tbuf[me]

    def send_route(t):
        peer = (me + t) % count
        remote(rbuf.at[peer], rww.at[me], rt_s, rt_r, ep=peer).start()

    loop(1, count, send_route)
    rww[me] = rbuf[me]

    small[4].wait()
    small[5].wait()
    gates = 2 * heads
    once = jnp.concatenate((wi[...].astype(f32), wf[...].astype(f32)), axis=0)
    thin = jnp.concatenate(
        (once, once, jnp.zeros((lanes - 2 * gates, width), f32)), axis=0
    ).astype(bf16)

    with jax.named_scope("normed"):
        others = nland.at[pl.ds(0, count - 1)]
        remote(others, others, p1_s, p1_r, ep=me).wait_recv()
    columns = nland[...].reshape(rows, width)

    lane = lax.broadcasted_iota(jnp.int32, (rows, lanes), 1)
    thin_sums = lax.dot_general(
        columns, thin, (((1,), (1,)), ((), ())), preferred_element_type=f32
    )
    upper = thin_sums.astype(bf16).astype(f32)
    parted = jnp.where(lane < gates, upper, thin_sums - upper).astype(bf16)
    pg[...] = parted.reshape(outer, inner, sequences, lanes)

    def send_gates(t):
        spot = place.spot(t)
        remote(
            pg.at[:, spot], gland1.at[n], g1_s, g1_r, ep=place.at(o, spot)
        ).start()

    loop(1, inner, send_gates)

    def send_part(h, plane):
        def send(t):
            spot = place.spot(t)
            remote(
                pbuf.at[h, plane, spot],
                land1.at[h, plane, n],
                l1_s,
                l1_r.at[h * outer + plane],
                ep=place.at(o, spot),
            ).start()

        loop(1, inner, send)

    for h in range(heads):
        for copy in wide_copies(h):
            copy.wait()
        sums = jnp.dot(columns, wide[h], preferred_element_type=f32).astype(bf16)
        pbuf[h] = sums.reshape(outer, inner, sequences, 4 * size)
        loop(1, outer, lambda t: send_part(h, place.plane(t)))
        if h > 0:
            send_part(h - 1, o)
    send_part(heads - 1, o)
    for copy in small[6:]:
        copy.wait()

    with jax.named_scope("gates"):
        others = gland1.at[pl.ds(0, inner - 1)]
        remote(others, others, g1_s, g1_r, ep=me).wait_recv()
    for a in range(outer):
        total = pg[a, n].astype(f32)
        for t in range(1, inner):
            total += gland1[place.spot(t), a].astype(f32)
        gmid[a] = total

    def pass_gates(t):
        plane = place.plane(t)
        remote(
            gmid.at[plane], gland2.at[o], g2_s, g2_r, ep=place.at(plane, n)
        ).start()

    loop(1, outer, pass_gates)

    def plane_sum(h, plane):
        with jax.named_scope("first"):
            others = land1.at[h, plane, pl.ds(0, inner - 1)]
            remote(others, others, l1_s, l1_r.at[h * outer + plane], ep=me).wait_recv()
        total = pbuf[h, plane, n].astype(f32)
        for t in range(1, inner):
            total += land1[h, plane, place.spot(t)].astype(f32)
        return total

    def first_sum(h):
        def send(t):
            plane = place.plane(t)
            total = plane_sum(h, plane)
            mid[h, plane] = total[:, : 2 * size]
            mid_half[h, plane] = total[:, 2 * size :].astype(bf16)
            target = place.at(plane, n)
            remote(mid.at[h, plane], land2.at[h, o], l2_s, l2_r.at[h], ep=target).start()
            remote(
                mid_half.at[h, plane], land2_half.at[h, o], l3_s, l3_r.at[h], ep=target
            ).start()

        loop(1, outer, send)

    def gate_math():
        with jax.named_scope("gates2"):
            others = gland2.at[pl.ds(0, outer - 1)]
            remote(others, others, g2_s, g2_r, ep=me).wait_recv()
        total = gmid[o]
        for t in range(1, outer):
            total += gland2[place.plane(t)]
        turn = jnp.transpose(total)
        turn = turn[:gates] + turn[gates : 2 * gates]
        input_pre, forget_pre = turn[:heads], turn[heads:]
        square = lax.broadcasted_iota(jnp.int32, (heads, heads), 0) == lax.broadcasted_iota(
            jnp.int32, (heads, heads), 1
        )
        shift = jnp.sum(jnp.where(square, bias[...], 0.0), axis=1, keepdims=True)
        shifted = forget_pre + shift
        log_forget = jnp.minimum(shifted, 0.0) - jnp.log1p(jnp.exp(-jnp.abs(shifted)))
        stab_new = jnp.maximum(log_forget + stab[...], input_pre)
        stab_out[...] = stab_new
        turned[...] = jnp.zeros_like(turned)
        turned[:heads, :sequences] = jnp.exp(log_forget + stab[...] - stab_new)
        turned[heads:gates, :sequences] = jnp.exp(input_pre - stab_new) * size**-0.5
        back = jnp.transpose(turned[...])[:sequences]
        for h in range(heads):
            carried_rows[h] = jnp.broadcast_to(back[:, h : h + 1], (sequences, lanes))
            written_rows[h] = jnp.broadcast_to(
                back[:, heads + h : heads + h + 1], (sequences, lanes)
            )

    def memory_head(h):
        own = plane_sum(h, o)
        with jax.named_scope("heads"):
            others = land2.at[h, pl.ds(0, outer - 1)]
            remote(others, others, l2_s, l2_r.at[h], ep=me).wait_recv()
            others = land2_half.at[h, pl.ds(0, outer - 1)]
            remote(others, others, l3_s, l3_r.at[h], ep=me).wait_recv()
        pltpu.make_async_copy(mem_in.at[:, h], mem.at[:, h], mi.at[h]).wait()
        query_key, value_gate = own[:, : 2 * size], own[:, 2 * size :]
        for t in range(1, outer):
            query_key += land2[h, place.plane(t)]
            value_gate += land2_half[h, place.plane(t)].astype(f32)
        query_key = query_key.astype(bf16)
        value_gate = value_gate.astype(bf16).astype(f32)
        query, key = query_key[:, :size], query_key[:, size:]
        value, outgate = value_gate[:, :size], value_gate[:, size:]
        value_columns = jnp.transpose(value)
        places = lax.broadcasted_iota(jnp.int32, (size, sequences), 1)
        slots = lax.broadcasted_iota(jnp.int32, (size, lanes), 1)
        query = query.astype(f32)
        carry, write = carried_rows[h], written_rows[h]
        answers = jnp.zeros((size, lanes), f32)
        for s in range(sequences):
            column = jnp.where(places == s, value_columns, 0.0).astype(bf16)
            product = jnp.dot(column, key, preferred_element_type=f32)
            updated = carry[s : s + 1, :] * mem[s, h] + write[s : s + 1, :] * product
            mem[s, h] = updated
            answer = jnp.sum(updated * query[s : s + 1, :], axis=1, keepdims=True)
            answers = jnp.where(slots == s, answer, answers)
        readout = jnp.transpose(answers)[:sequences]
        mean_square = jnp.mean(readout * readout, axis=-1, keepdims=True)
        gated = (
            readout
            * lax.rsqrt(mean_square + norm_eps)
            * hgain[pl.ds(h, 1), :]
            * sigmoid(outgate)
        )
        gland[h, me] = gated.astype(bf16)
        block = gland.at[h, me]
        loop(
            1,
            outer,
            lambda t: remote(
                block, block, ag_s, ag_r.at[h], ep=place.at(place.plane(t), n)
            ).start(),
        )
        if not planar:
            loop(
                1,
                inner,
                lambda u: remote(
                    block, block, ag_s, ap_r.at[h], ep=place.at(o, place.spot(u))
                ).start(),
            )

    def relay(h):
        others = gland.at[h, pl.ds(0, outer - 1)]
        remote(others, others, ag_s, ag_r.at[h], ep=me).wait_recv()

        def one(t):
            block = gland.at[h, place.at(place.plane(t), n)]
            loop(
                1,
                inner,
                lambda u: remote(
                    block, block, ag_s, ap_r.at[h], ep=place.at(o, place.spot(u))
                ).start(),
            )

        loop(1, outer, one)

    def head_step(h):
        @pl.when(h < heads)
        def _():
            first_sum(h)

        @pl.when(h == 0)
        def _():
            gate_math()

        if planar:

            @pl.when(h == heads)
            def _():
                loop(
                    1,
                    inner,
                    lambda u: remote(
                        mix, mixp.at[n], mx_s, mx_r, ep=place.at(o, place.spot(u))
                    ).start(),
                )

        @pl.when(h > 0)
        def _():
            memory_head(h - 1)

    loop(0, heads + 1, head_step)

    def together():
        with jax.named_scope("gated"):
            mixp[n] = mix[...]
            lines = []
            for h in range(heads):
                others = gland.at[h, pl.ds(0, outer - 1)]
                remote(others, others, ag_s, ag_r.at[h], ep=me).wait_recv()
                lines.append(
                    jnp.concatenate([gland[h, place.at(a, n)] for a in range(outer)], axis=0)
                )
            lines = jnp.concatenate(lines, axis=1)
            others = mixp.at[pl.ds(0, inner - 1)]
            remote(others, others, mx_s, mx_r, ep=me).wait_recv()
            for i in range(inner):
                pv[i // part_spots, i % part_spots] = jnp.dot(
                    lines, mixp[i], preferred_element_type=f32
                ).astype(bf16)
        swap = remote(pv.at[sibling], came, tp_s, tp_r, tp=sibling)
        swap.start()
        others = tland.at[pl.ds(0, outer - 1)]
        remote(others, others, tk_s, tk_r.at[0], ep=me).wait_recv()
        with jax.named_scope("swap"):
            swap.wait_recv()
        for i in range(part_spots):
            attended = pv[side, i].astype(f32) + came[i].astype(f32)
            base = (o * inner + side * part_spots + i) * width
            for a in range(outer):
                lower = a * sequences
                res[a, n, :, pl.ds(pl.multiple_of(base, width), width)] = (
                    tland[a, i].astype(f32) + attended[lower : lower + sequences]
                ).astype(bf16)
        return swap

    def apart():
        with jax.named_scope("gated"):
            loop(0, heads, relay)
            partial = jnp.zeros((rows, width), f32)
            for h in range(heads):
                others = gland.at[h, pl.ds(0, outer * (inner - 1))]
                remote(others, others, ag_s, ap_r.at[h], ep=me).wait_recv()
                partial += jnp.dot(
                    gland[h].reshape(rows, size),
                    mix[h * size : (h + 1) * size, :],
                    preferred_element_type=f32,
                )
            partial = partial.astype(bf16)
        pv[...] = partial.reshape(2, half, width)
        swap = remote(pv.at[sibling], came, tp_s, tp_r, tp=sibling)
        swap.start()

        def take_tokens(b):
            source = side * per_half + b

            @pl.when(source != me)
            def _():
                remote(tland.at[b], tland.at[b], tk_s, tk_r.at[b], ep=source).wait_recv()

        loop(0, per_half, take_tokens)
        with jax.named_scope("swap"):
            swap.wait_recv()
        attended = pv[side].astype(f32) + came[...].astype(f32)
        residual = (tland[...].reshape(half, width).astype(f32) + attended).astype(bf16)
        res[me, side] = residual
        return swap

    swap = together() if planar else apart()

    def slot(p, core):
        if planar:
            base = (p // inner * inner + core * part_spots) * width
            return res.at[
                :, p % inner, :, pl.ds(pl.multiple_of(base, width), part_spots * width)
            ]
        return res.at[p, core]

    def hand(p):
        remote(slot(p, side), slot(p, side), sb_s, sb_r.at[p // inner], tp=sibling).start()

    def complete(t):
        plane = place.plane(t)
        if planar:
            base = (plane * inner + sibling * part_spots) * width
            whole = res.at[:, :, :, pl.ds(pl.multiple_of(base, width), part_spots * width)]
        else:
            whole = res.at[pl.ds(plane * inner, inner), sibling]
        with jax.named_scope("settle"):
            remote(whole, whole, sb_s, sb_r.at[plane], tp=sibling).wait_recv()
        if group is not None:
            group(plane)

    ready()
    others = rww.at[pl.ds(0, count - 1)]
    remote(others, others, rt_s, rt_r, ep=me).wait()
    with jax.named_scope("rows"):
        gather(place, lambda p: slot(p, side), ar_s, ar_p, ar_r, hand, complete)

    def settle():
        if planar:
            block = part_spots * width
            whole = res.at[:, :, :, pl.ds(0, outer * block)]
            sent = res.at[:, pl.ds(0, outer - 1), :, pl.ds(0, block)]
            passed = res.at[:, pl.ds(0, inner - 1), :, pl.ds(0, outer * block)]
        else:
            whole, sent = res.at[:, side], res.at[pl.ds(0, outer - 1), side]
            passed = res.at[pl.ds(0, outer * (inner - 1)), side]
        remote(whole, whole, sb_s, sb_r.at[0], tp=sibling).wait_send()
        remote(sent, sent, ar_s, ar_r.at[0], ep=me).wait_send()
        remote(passed, passed, ar_p, ar_r.at[0], ep=me).wait_send()
        others = nbuf.at[pl.ds(0, count - 1)]
        remote(others, others, p1_s, p1_r, ep=me).wait_send()

        if planar:
            others = tland.at[pl.ds(0, outer - 1)]
            remote(others, others, tk_s, tk_r.at[0], ep=me).wait_send()
            others = mixp.at[pl.ds(0, inner - 1)]
            remote(others, others, mx_s, mx_r, ep=me).wait_send()
        else:

            @pl.when(mine)
            def _():
                remote(others, others, tk_s, tk_r.at[0], ep=me).wait_send()

        others = gland1.at[pl.ds(0, inner - 1)]
        remote(others, others, g1_s, g1_r, ep=me).wait_send()
        others = gmid.at[pl.ds(0, outer - 1)]
        remote(others, others, g2_s, g2_r, ep=me).wait_send()
        others = pbuf.at[:, :, pl.ds(0, inner - 1)]
        remote(others, others, l1_s, l1_r.at[0], ep=me).wait_send()
        others = mid.at[:, pl.ds(0, outer - 1)]
        remote(others, others, l2_s, l2_r.at[0], ep=me).wait_send()
        others = mid_half.at[:, pl.ds(0, outer - 1)]
        remote(others, others, l3_s, l3_r.at[0], ep=me).wait_send()
        others = gland.at[:, pl.ds(0, (outer if planar else count) - 1)]
        remote(others, others, ag_s, ag_r.at[0], ep=me).wait_send()
        swap.wait_send()

    return settle


def second_kernel(
    outer,
    inner,
    chunks,
    row_blocks,
    res,
    rww,
    gain_in,
    scale_in,
    wg,
    wu,
    wd,
    dg,
    du,
    dd,
    out,
    gain,
    scale,
    wgv,
    wuv,
    wdv,
    dgv,
    duv,
    ddv,
    gate_sum,
    up_sum,
    dense_gate_sum,
    dense_up_sum,
    squares,
    dense_act,
    row_weight,
    act,
    passed,
    landed,
    kept,
    summed,
    land1,
    mid,
    land2,
    wg_m,
    wu_m,
    wd_m,
    d_m,
    tp_s,
    tp_r,
    l1_s,
    l1_r,
    l2_s,
    l2_r,
):
    place = Place(outer, inner)
    me, side, o, n = place.me, place.side, place.o, place.n
    count = outer * inner
    rows, model_width = act.shape[0], res.shape[-1]
    sequences = rows // count
    sibling = 1 - side
    hidden_chunk = wgv.shape[2]
    column_chunk = wdv.shape[2]
    part_width = chunks * column_chunk

    dense = [
        pltpu.make_async_copy(source, target, d_m.at[i])
        for i, (source, target) in enumerate(
            ((dg, dgv), (du, duv), (dd, ddv), (gain_in, gain), (scale_in, scale))
        )
    ]
    hidden_chunks = wgv.shape[0]

    def gate_copy(c):
        span = pl.ds(c * hidden_chunk, hidden_chunk)
        return pltpu.make_async_copy(wg.at[0, :, span], wgv.at[c], wg_m.at[c])

    def up_copy(c):
        span = pl.ds(c * hidden_chunk, hidden_chunk)
        return pltpu.make_async_copy(wu.at[0, :, span], wuv.at[c], wu_m.at[c])

    def down_copy(c):
        span = pl.ds(c * column_chunk, column_chunk)
        return pltpu.make_async_copy(wd.at[0, :, span], wdv.at[c], wd_m.at[c])

    block = act.shape[0] // row_blocks
    across = model_width // outer

    def part(r):
        return pl.ds(pl.multiple_of(r * block, block), block)

    def begin():
        dense[3].start()
        for c in range(hidden_chunks):
            gate_copy(c).start()
            up_copy(c).start()
        for c in (0, 1, 2, 4):
            dense[c].start()
        for c in range(chunks):
            down_copy(sibling * chunks + c).start()
            down_copy(side * chunks + c).start()
        for sums in (gate_sum, up_sum, dense_gate_sum, dense_up_sum, squares):
            sums[...] = jnp.zeros_like(sums)

    def arrive():
        dense[3].wait()
        dense[0].wait()
        dense[1].wait()
        for c in range(hidden_chunks):
            gate_copy(c).wait()
            up_copy(c).wait()

    turned = (((1,), (1,)), ((), ()))

    def group(plane):
        span = pl.ds(pl.multiple_of(plane * across, across), across)

        def one(r):
            if len(res.shape) == 4:
                values = res[:, :, :, span].reshape(rows, across).astype(f32)
            else:
                values = res[part(r), span].astype(f32)
            squares[part(r), :] += jnp.sum(values * values, axis=-1, keepdims=True)
            scaled = (values * gain[:, span]).astype(bf16)
            for c in range(hidden_chunks):
                gate_sum[c, part(r), :] += jnp.dot(
                    scaled, wgv[c, span, :], preferred_element_type=f32
                )
                up_sum[c, part(r), :] += jnp.dot(
                    scaled, wuv[c, span, :], preferred_element_type=f32
                )
            dense_gate_sum[part(r), :] += lax.dot_general(
                scaled, dgv[:, span], turned, preferred_element_type=f32
            )
            dense_up_sum[part(r), :] += lax.dot_general(
                scaled, duv[:, span], turned, preferred_element_type=f32
            )

        with jax.named_scope("group"):
            loop(0, row_blocks, one)

    def products():
        received = jnp.broadcast_to(rww[...], (count, sequences, lanes)).reshape(rows, lanes)
        line = lax.broadcasted_iota(jnp.int32, (rows, lanes), 0) % sequences
        lane = lax.broadcasted_iota(jnp.int32, (rows, lanes), 1)
        row_weight[...] = jnp.sum(jnp.where(line == lane, received, 0.0), axis=-1, keepdims=True)

        row_scale = lax.rsqrt(squares[...] / model_width + norm_eps)
        squares[...] = row_scale

        def activate(r):
            scale_rows = squares[part(r), :]
            gate_rows = dense_gate_sum[part(r), :] * scale_rows
            lift_rows = dense_up_sum[part(r), :] * scale_rows
            dense_act[part(r), :] = (gate_rows * sigmoid(gate_rows) * lift_rows).astype(bf16)
            for c in range(hidden_chunks):
                gate_pre = jnp.minimum(gate_sum[c, part(r), :] * scale_rows, clamp_limit)
                up_pre = jnp.clip(up_sum[c, part(r), :] * scale_rows, -clamp_limit, clamp_limit)
                act[part(r), c * hidden_chunk : (c + 1) * hidden_chunk] = (
                    (up_pre + 1.0) * gate_pre * sigmoid(sigmoid_slope * gate_pre)
                ).astype(bf16)

        with jax.named_scope("hidden"):
            loop(0, row_blocks, activate)

        dense[2].wait()
        dense[4].wait()

        def term(c, r):
            span = pl.ds(pl.multiple_of(c * column_chunk, column_chunk), column_chunk)
            routed = jnp.dot(act[part(r), :], wdv[c], preferred_element_type=f32)
            dense_out = jnp.dot(dense_act[part(r), :], ddv[:, span], preferred_element_type=f32)
            return dense_out * scale[:, span] + row_weight[part(r), :] * routed

        def cross(c):
            return remote(passed.at[c], landed.at[c], tp_s, tp_r.at[c], tp=sibling)

        def spread_plane(c, plane):
            def send(t):
                spot = place.spot(t)
                remote(
                    summed.at[c, plane, spot],
                    land1.at[c, plane, n],
                    l1_s,
                    l1_r.at[c * outer + plane],
                    ep=place.at(o, spot),
                ).start()

            loop(1, inner, send)

        def spread(c):
            cross(c).wait_recv()
            both = kept[c] + landed[c].astype(f32)
            summed[c] = both.astype(bf16).reshape(outer, inner, sequences, column_chunk)

            loop(1, outer, lambda t: spread_plane(c, place.plane(t)))

        def give_step(c):
            down_copy(sibling * chunks + c).wait()

            def give(r):
                passed[c, part(r), :] = term(sibling * chunks + c, r).astype(bf16)

            loop(0, row_blocks, give)
            cross(c).start()

        def keep_step(c):
            down_copy(side * chunks + c).wait()

            def keep(r):
                kept[c, part(r), :] = term(side * chunks + c, r)

            loop(0, row_blocks, keep)
            spread(c)

        with jax.named_scope("give"):
            give_step(0)

            def turn(c):
                give_step(c)
                keep_step(c - 1)

            loop(1, chunks, turn)
        with jax.named_scope("keep"):
            keep_step(chunks - 1)

        loop(0, chunks, lambda c: spread_plane(c, o))

        def plane_sum(c, plane):
            others = land1.at[c, plane, pl.ds(0, inner - 1)]
            remote(others, others, l1_s, l1_r.at[c * outer + plane], ep=me).wait_recv()
            total = summed[c, plane, n].astype(f32)
            for t in range(1, inner):
                total += land1[c, plane, place.spot(t)].astype(f32)
            return total

        def first_sum(c):
            def send(t):
                plane = place.plane(t)
                mid[c, plane] = plane_sum(c, plane).astype(bf16)
                remote(
                    mid.at[c, plane], land2.at[c, o], l2_s, l2_r.at[c], ep=place.at(plane, n)
                ).start()

            loop(1, outer, send)

        with jax.named_scope("sum1"):
            loop(0, chunks, first_sum)

        columns = pl.ds(pl.multiple_of(side * part_width, part_width), part_width)
        if len(res.shape) == 4:
            residual = res[o, n, :, columns].astype(f32)
        else:
            own_rows = pl.ds(pl.multiple_of(me * sequences, sequences), sequences)
            residual = res[own_rows, columns].astype(f32)

        with jax.named_scope("sum2"):
            for c in range(chunks):
                total = plane_sum(c, o)
                others = land2.at[c, pl.ds(0, outer - 1)]
                remote(others, others, l2_s, l2_r.at[c], ep=me).wait_recv()
                for t in range(1, outer):
                    total += land2[c, place.plane(t)].astype(f32)
                span = slice(c * column_chunk, (c + 1) * column_chunk)
                out[:, span] = (residual[:, span] + total).astype(bf16)

    def settle():
        remote(passed, landed, tp_s, tp_r.at[0], tp=sibling).wait_send()
        others = summed.at[:, :, pl.ds(0, inner - 1)]
        remote(others, others, l1_s, l1_r.at[0], ep=me).wait_send()
        others = mid.at[:, pl.ds(0, outer - 1)]
        remote(others, others, l2_s, l2_r.at[0], ep=me).wait_send()

    def finish():
        products()
        return settle

    return begin, arrive, group, finish


def alone_kernel(outer, inner, *refs):
    first_kernel(outer, inner, *refs)()


def experts_kernel(outer, inner, chunks, row_blocks, *refs):
    place = Place(outer, inner)
    barrier = pltpu.get_barrier_semaphore()
    loop(1, inner, lambda u: greet(barrier, ep=place.at(place.o, place.spot(u))))
    loop(1, outer, lambda t: greet(barrier, ep=place.at(place.plane(t), place.n)))
    greet(barrier, tp=1 - place.side)
    begin, arrive, group, finish = second_kernel(outer, inner, chunks, row_blocks, *refs)
    begin()
    arrive()
    loop(0, outer, group)
    pl.semaphore_wait(barrier, inner + outer - 1)
    finish()()


def whole_kernel(outer, inner, chunks, row_blocks, firsts, *refs):
    first_in, second_in, refs = refs[:15], refs[15:23], refs[23:]
    (mixed, stab_out, mem), (res, rww), refs = refs[:3], refs[3:5], refs[5:]
    begin, arrive, group, finish = second_kernel(
        outer, inner, chunks, row_blocks, res, rww, *second_in, mixed, *refs[firsts:]
    )
    settle = first_kernel(
        outer,
        inner,
        *first_in,
        res,
        rww,
        stab_out,
        mem,
        *refs[:firsts],
        planar=True,
        begin=begin,
        ready=arrive,
        group=group,
    )
    finish()()
    settle()


def last_kernel(mixed_in, memory_in, stab_in, mixed, memory, stab, sems):
    parts = sems.shape[0] - 2
    each = memory.shape[0] // parts
    pairs = [(mixed_in, mixed), (stab_in, stab)]
    for part in range(parts):
        span = pl.ds(part * each, each)
        pairs.append((memory_in.at[span], memory.at[span]))
    moves = [
        pltpu.make_async_copy(source, target, sems.at[i])
        for i, (source, target) in enumerate(pairs)
    ]
    for move in moves:
        move.start()
    for move in moves:
        move.wait()


def in_vmem():
    return pl.BlockSpec(memory_space=pltpu.VMEM)


def in_place():
    return pl.BlockSpec(memory_space=pltpu.HBM)


def held(*arrays):
    return [pltpu.with_memory_space_constraint(array, pltpu.HBM) for array in arrays]


def copies(*numbers):
    return [
        pltpu.SemaphoreType.DMA((number,)) if number else pltpu.SemaphoreType.DMA
        for number in numbers
    ]


def body(
    tokens,
    norm_gain,
    query_weight,
    key_weight,
    value_weight,
    outgate_weight,
    input_weight,
    forget_weight,
    forget_bias,
    memory,
    stabilizer,
    head_gain,
    mix_weight,
    second_gain,
    route_experts,
    route_weight,
    expert_gate,
    expert_up,
    expert_down,
    dense_gate,
    dense_up,
    dense_down,
    branch_scale,
):
    sequences, model_width = tokens.shape
    count = lax.axis_size("ep")
    sides = lax.axis_size("tp")
    inner = 1 << ((count.bit_length() - 1) // 2)
    outer = count // inner
    rows = sequences * count
    half = rows // sides
    width = model_width // count
    heads, size = memory.shape[1], memory.shape[2]
    head_width = query_weight.shape[1]
    part_width = model_width // sides
    topk = route_experts.shape[1]

    aligned = width % lanes == 0
    landing = (sides, half, model_width) if aligned else (count, sides, half, width)
    gates = 2 * heads
    grown = rows // 256

    hidden = expert_gate.shape[2]
    dense_rows = dense_gate.shape[0]
    hidden_chunk = min(hidden, 256)
    column_chunk = min(part_width, 256)
    chunks = part_width // column_chunk
    row_blocks = 1 if aligned else max(1, grown)
    token_landing = (count // sides, sequences, width)
    part_shape = (half, width)
    if aligned:
        token_landing = (outer, inner // sides, sequences, width)
        part_shape = (inner // sides, outer * sequences, width)
    first_scratch = [
        pltpu.VMEM((sequences, model_width), bf16),
        pltpu.VMEM((1, model_width), f32),
        pltpu.VMEM((heads, width, 4 * size), bf16),
        pltpu.VMEM((heads, width), bf16),
        pltpu.VMEM((heads, width), bf16),
        pltpu.VMEM((1, heads), f32),
        pltpu.VMEM((heads, sequences), f32),
        pltpu.VMEM((heads, size), f32),
        pltpu.VMEM((head_width, width), bf16),
        pltpu.VMEM((topk, sequences), jnp.int32),
        pltpu.VMEM((topk, sequences), f32),
        pltpu.VMEM((count, sequences, width), bf16),
        pltpu.VMEM((count, sequences, width), bf16),
        pltpu.VMEM((count, sequences, width), bf16),
        pltpu.VMEM(token_landing, bf16),
        pltpu.VMEM((count, 1, lanes), f32),
        pltpu.VMEM((outer, inner, sequences, lanes), bf16),
        pltpu.VMEM((inner, outer, sequences, lanes), bf16),
        pltpu.VMEM((outer, sequences, lanes), f32),
        pltpu.VMEM((outer, sequences, lanes), f32),
        pltpu.VMEM((heads, outer, inner, sequences, 4 * size), bf16),
        pltpu.VMEM((heads, outer, inner, sequences, 4 * size), bf16),
        pltpu.VMEM((heads, outer, sequences, 2 * size), f32),
        pltpu.VMEM((heads, outer, sequences, 2 * size), f32),
        pltpu.VMEM((heads, outer, sequences, 2 * size), bf16),
        pltpu.VMEM((heads, outer, sequences, 2 * size), bf16),
        pltpu.VMEM((gates, lanes), f32),
        pltpu.VMEM((heads, sequences, lanes), f32),
        pltpu.VMEM((heads, sequences, lanes), f32),
        pltpu.VMEM((heads, count, sequences, size), bf16),
        pltpu.VMEM((sides,) + part_shape, bf16),
        pltpu.VMEM(part_shape, bf16),
        pltpu.VMEM((inner, head_width, width), bf16),
    ]
    first_scratch += copies(10, 4 * heads)
    first_scratch += copies(0, 0, 0, count // sides, 0, 0, 0, 0, 0, 0)
    first_scratch += copies(0, heads * outer, 0, heads, 0, heads, heads)
    first_scratch += copies(0, heads, heads, 0, 0, 0, count, 0, outer, 0, 0, 0)
    second_scratch = [
        pltpu.VMEM((1, model_width), f32),
        pltpu.VMEM((1, model_width), f32),
        pltpu.VMEM((hidden // hidden_chunk, model_width, hidden_chunk), bf16),
        pltpu.VMEM((hidden // hidden_chunk, model_width, hidden_chunk), bf16),
        pltpu.VMEM((2 * chunks, hidden, column_chunk), bf16),
        pltpu.VMEM((dense_rows, model_width), bf16),
        pltpu.VMEM((dense_rows, model_width), bf16),
        pltpu.VMEM((dense_rows, model_width), bf16),
        pltpu.VMEM((hidden // hidden_chunk, rows, hidden_chunk), f32),
        pltpu.VMEM((hidden // hidden_chunk, rows, hidden_chunk), f32),
        pltpu.VMEM((rows, dense_rows), f32),
        pltpu.VMEM((rows, dense_rows), f32),
        pltpu.VMEM((rows, 1), f32),
        pltpu.VMEM((rows, dense_rows), bf16),
        pltpu.VMEM((rows, 1), f32),
        pltpu.VMEM((rows, hidden), bf16),
        pltpu.VMEM((chunks, rows, column_chunk), bf16),
        pltpu.VMEM((chunks, rows, column_chunk), bf16),
        pltpu.VMEM((chunks, rows, column_chunk), f32),
        pltpu.VMEM((chunks, outer, inner, sequences, column_chunk), bf16),
        pltpu.VMEM((chunks, outer, inner, sequences, column_chunk), bf16),
        pltpu.VMEM((chunks, outer, sequences, column_chunk), bf16),
        pltpu.VMEM((chunks, outer, sequences, column_chunk), bf16),
    ]
    second_scratch += copies(hidden // hidden_chunk, hidden // hidden_chunk, 2 * chunks, 5)
    second_scratch += copies(0, chunks, 0, chunks * outer, 0, chunks)
    first_arguments = held(
        tokens,
        norm_gain.reshape(1, model_width),
        query_weight,
        key_weight,
        value_weight,
        outgate_weight,
        input_weight.T,
        forget_weight.T,
        forget_bias.reshape(1, heads),
        stabilizer.T,
        head_gain.reshape(heads, size),
        mix_weight,
        route_experts.T,
        route_weight.T,
        memory,
    )
    second_arguments = held(
        second_gain.reshape(1, model_width),
        branch_scale.reshape(1, model_width),
        expert_gate,
        expert_up,
        expert_down,
        dense_gate,
        dense_up,
        dense_down,
    )
    mixed_shape = jax.ShapeDtypeStruct((sequences, part_width), bf16)
    stab_shape = jax.ShapeDtypeStruct((heads, sequences), f32)
    memory_shape = jax.ShapeDtypeStruct(memory.shape, f32)
    if aligned:
        mixed, stab_new, memory_new = pl.pallas_call(
            functools.partial(
                whole_kernel, outer, inner, chunks, row_blocks, len(first_scratch)
            ),
            out_shape=(mixed_shape, stab_shape, memory_shape),
            in_specs=[in_place()] * 23,
            out_specs=(in_vmem(),) * 3,
            scratch_shapes=[
                pltpu.VMEM((outer, inner, sequences, model_width), bf16),
                pltpu.VMEM((count, 1, lanes), f32),
            ]
            + first_scratch
            + second_scratch,
            compiler_params=pltpu.CompilerParams(
                collective_id=1, has_side_effects=True, vmem_limit_bytes=44 * 2**20
            ),
        )(*first_arguments, *second_arguments)
    else:
        residual, row_weights, stab_new, memory_new = pl.pallas_call(
            functools.partial(alone_kernel, outer, inner),
            out_shape=(
                jax.ShapeDtypeStruct((count, sides, half, width), bf16),
                jax.ShapeDtypeStruct((count, 1, lanes), f32),
                stab_shape,
                memory_shape,
            ),
            in_specs=[in_place()] * 15,
            out_specs=(in_vmem(),) * 4,
            scratch_shapes=first_scratch,
            compiler_params=pltpu.CompilerParams(
                collective_id=1, has_side_effects=True, vmem_limit_bytes=46 * 2**20
            ),
        )(*first_arguments)
        residual = residual.transpose(1, 2, 0, 3).reshape(rows, model_width)
        mixed = pl.pallas_call(
            functools.partial(experts_kernel, outer, inner, chunks, row_blocks),
            out_shape=mixed_shape,
            in_specs=[in_vmem()] * 2 + [in_place()] * 8,
            out_specs=in_vmem(),
            scratch_shapes=second_scratch,
            compiler_params=pltpu.CompilerParams(
                collective_id=2, has_side_effects=True, vmem_limit_bytes=56 * 2**20
            ),
        )(residual, row_weights, *second_arguments)

    mixed, memory_new, stab_new = pl.pallas_call(
        last_kernel,
        out_shape=tuple(
            jax.ShapeDtypeStruct(array.shape, array.dtype)
            for array in (mixed, memory_new, stab_new)
        ),
        in_specs=[in_vmem()] * 3,
        out_specs=(in_place(),) * 3,
        scratch_shapes=copies(2 + min(sequences, 8)),
        compiler_params=pltpu.CompilerParams(vmem_limit_bytes=8 * 2**20),
    )(mixed, memory_new, stab_new)
    return (mixed, memory_new, stab_new.T)


def solution(mesh):
    in_specs = (
        P("ep", None),
        P(),
        P("ep", "tp"),
        P("ep", "tp"),
        P("ep", "tp"),
        P("ep", "tp"),
        P("ep", "tp"),
        P("ep", "tp"),
        P("tp"),
        P("ep", "tp", None, None),
        P("ep", "tp"),
        P("tp"),
        P("tp", "ep"),
        P(),
        P("ep", None),
        P("ep", None),
        P("ep", None, "tp"),
        P("ep", None, "tp"),
        P("ep", "tp", None),
        P(("ep", "tp"), None),
        P(("ep", "tp"), None),
        P(("ep", "tp"), None),
        P(),
    )
    out_specs = (P("ep", "tp"), P("ep", "tp", None, None), P("ep", "tp"))
    return jax.shard_map(body, mesh=mesh, in_specs=in_specs, out_specs=out_specs, check_vma=False)
```
